256 devices in a mesh: grp: 4 (over y, x), tp: 64 (over z, core).
Axes of the slice: x: 2, y: 2, z: 32, core: 2. Of those that a mesh axis runs over, the one named last changes fastest.
The devices are a block of a 4x8x32 slice.
Arguments:
- tokens: bfloat16 [256, 2048], P('grp'), parts along dimension 0, may hold values from -6 to 6
- norm_gain: float32 [2, 2048], replicated, may hold values from 0.1 to 1.9
- query_weight: bfloat16 [2, 2048, 2048], P(None, 'tp'), may hold values from -0.125 to 0.125
- key_weight: bfloat16 [2, 2048, 2048], P(None, 'tp'), may hold values from -0.125 to 0.125
- value_weight: bfloat16 [2, 2048, 2048], P(None, 'tp'), may hold values from -0.125 to 0.125
- outgate_weight: bfloat16 [2, 2048, 2048], P(None, 'tp'), may hold values from -0.125 to 0.125
- gate_weight: bfloat16 [2, 2048, 16], replicated, may hold values from -0.125 to 0.125
- forget_bias: float32 [2, 8], replicated, may hold values from 0 to 4
- proj_weight: bfloat16 [2, 2048, 2048], P(None, 'tp'), may hold values from -0.125 to 0.125
- cell_state: float32 [2, 256, 2048, 256], P(None, 'grp', 'tp'), parts along dimension 1, may hold values from -0.3 to 0.3
- normalizer: float32 [2, 256, 2048], P(None, 'grp', 'tp'), parts along dimension 1, may hold values from -0.3 to 0.3
- stabilizer: float32 [2, 256, 8], P(None, 'grp'), parts along dimension 1, may hold values from -2 to 2
Outputs:
- mixed: bfloat16 [256, 2048], P('grp', 'tp'), parts along dimension 0
- new_cell: float32 [2, 256, 2048, 256], P(None, 'grp', 'tp'), parts along dimension 1
- new_normalizer: float32 [2, 256, 2048], P(None, 'grp', 'tp'), parts along dimension 1
- new_stabilizer: float32 [2, 256, 8], P(None, 'grp'), parts along dimension 1
The draws below stay inside these ranges and needn't reach their ends.
There are 4 independent parts, one for each index of `grp`. The reference program is written for one: setup_inputs(seed, part) draws one part's arguments, and reference() takes and returns one part's arrays. A program takes and returns all parts, laid end to end along the dimension named above; an argument that names none is the same for every part. Nothing has to cross between parts.
All inputs are finite; a program needn't handle non-finite values.
Results may differ from the reference program's by a relative error of at most 0.025.
Values may be sent and summed in bfloat16 or wider, within the bound.
No kernel may reach another device: no remote copies, remote signals or barrier semaphores. Data moves between devices by JAX's collectives and lax.ppermute only.
A program may use at most 64 MiB of HBM per device.

```python
import jax
import jax.numpy as jnp
from jax import lax

D = 2048
DH = 256
HEADS = 8
LAYERS = 2
BATCH = 64


def block_levels(rng, dims, split, low, largest):
    loudness = 1.0
    for axis_at, parts in split:
        heights = jax.random.uniform(jax.random.fold_in(jax.random.fold_in(rng, 6), axis_at), (parts,), jnp.float32, low / len(split), largest / len(split))
        loudness = loudness * jnp.repeat(jnp.exp(heights), dims[axis_at] // parts).reshape((-1,) + (1,) * (len(dims) - 1 - axis_at))
    return loudness


def centred(key, shape, width, most, shards=(), kind=jnp.bfloat16):
    entries = jax.random.normal(key, shape, jnp.float32) * width
    if len(shards) > 0:
        entries = block_levels(key, shape, shards, -0.22, 0.18) * entries
    return jnp.clip(entries, min=-most, max=most).astype(kind)


def setup_inputs(seed: int = 0, part: int = 0) -> dict:
    key_list = jax.random.split(jax.random.key(seed), 13)
    own_keys = jax.random.split(jax.random.fold_in(key_list[12], part), 13)
    tokens = centred(own_keys[0], (BATCH, D), 1.0, 6.0)
    norm_gain = jnp.clip(1.0 + 0.18 * jax.random.normal(key_list[1], (LAYERS, D), jnp.float32), 0.1, 1.9)
    query_weight = centred(key_list[2], (LAYERS, D, D), D ** -0.5, 0.125, ((1, 64),))
    key_weight = centred(key_list[3], (LAYERS, D, D), D ** -0.5, 0.125, ((1, 64),))
    value_weight = centred(key_list[4], (LAYERS, D, D), D ** -0.5, 0.125, ((1, 64),))
    outgate_weight = centred(key_list[5], (LAYERS, D, D), D ** -0.5, 0.125, ((1, 64),))
    gate_weight = centred(key_list[6], (LAYERS, D, 2 * HEADS), D ** -0.5, 0.125)
    forget_bias = jnp.clip(jax.random.uniform(key_list[7], (LAYERS, HEADS), jnp.float32, 0.0, 4.0), 0.0, 4.0)
    proj_weight = centred(key_list[8], (LAYERS, D, D), D ** -0.5, 0.125, ((1, 64),))
    cell_state = centred(own_keys[9], (LAYERS, BATCH, D, DH), 0.05, 0.3, ((2, 64),), jnp.float32)
    normalizer = centred(own_keys[10], (LAYERS, BATCH, D), 0.05, 0.3, ((2, 64),), jnp.float32)
    stabilizer = jnp.clip(jax.random.uniform(own_keys[11], (LAYERS, BATCH, HEADS), jnp.float32, -2.0, 2.0), -2.0, 2.0)
    return {"tokens": tokens, "norm_gain": norm_gain, "query_weight": query_weight, "key_weight": key_weight, "value_weight": value_weight, "outgate_weight": outgate_weight, "gate_weight": gate_weight, "forget_bias": forget_bias, "proj_weight": proj_weight, "cell_state": cell_state, "normalizer": normalizer, "stabilizer": stabilizer}


epsilon = 1e-06

def project(normed, weight):
    return lax.dot_general(normed, weight, (((1,), (1,)), ((), ())), preferred_element_type=jnp.float32)

def one_cell(current, gain, w_query, w_key, w_value, w_outgate, w_gates, bias_forget, w_proj, cell, norm_vec, stab):
    batch = current.shape[0]
    heads = D // DH
    cur_f = current.astype(jnp.float32)
    normed = (cur_f * lax.rsqrt(lax.optimization_barrier(jnp.mean(cur_f * cur_f, axis=-1, keepdims=True)) + epsilon) * gain).astype(jnp.bfloat16)
    query = project(normed, w_query).astype(jnp.bfloat16)
    keys = (project(normed, w_key) * DH ** (-0.5)).astype(jnp.bfloat16)
    values = project(normed, w_value).astype(jnp.bfloat16)
    outgate = project(normed, w_outgate).astype(jnp.bfloat16)
    gates = jnp.dot(normed, w_gates, preferred_element_type=jnp.float32)
    in_gate = gates[:, :heads]
    log_forget = jax.nn.log_sigmoid(gates[:, heads:] + bias_forget)
    new_stab = jnp.maximum(log_forget + stab, in_gate)
    decay = jnp.exp(log_forget + stab - new_stab)
    weight_in = jnp.exp(in_gate - new_stab)
    q_heads = query.astype(jnp.float32).reshape(batch, heads, DH)
    k_heads = keys.astype(jnp.float32).reshape(batch, heads, DH)
    v_heads = values.astype(jnp.float32).reshape(batch, heads, DH)
    old_cell = cell.reshape(batch, heads, DH, DH)
    outer = v_heads[:, :, :, None] * k_heads[:, :, None, :]
    new_cell = decay[:, :, None, None] * old_cell + weight_in[:, :, None, None] * outer
    new_norm = decay[:, :, None] * norm_vec.reshape(batch, heads, DH) + weight_in[:, :, None] * k_heads
    numer = jnp.einsum('bhk,bhek->bhe', q_heads, new_cell, precision=lax.Precision.HIGHEST)
    denom = lax.optimization_barrier(jnp.sum(q_heads * new_norm, axis=-1))
    readout = numer / jnp.maximum(jnp.abs(denom), jnp.exp(-new_stab))[:, :, None]
    branch = (jax.nn.sigmoid(outgate.astype(jnp.float32)) * readout.reshape(batch, D)).astype(jnp.bfloat16)
    result = (cur_f + project(branch, w_proj)).astype(jnp.bfloat16)
    return (result, new_cell.reshape(batch, D, DH), new_norm.reshape(batch, D), new_stab)

def reference(tokens, norm_gain, query_weight, key_weight, value_weight, outgate_weight, gate_weight, forget_bias, proj_weight, cell_state, normalizer, stabilizer):
    current = tokens
    cells = []
    norms = []
    stabs = []
    for layer in range(LAYERS):
        current, new_cell, new_norm, new_stab = one_cell(current, norm_gain[layer], query_weight[layer], key_weight[layer], value_weight[layer], outgate_weight[layer], gate_weight[layer], forget_bias[layer], proj_weight[layer], cell_state[layer], normalizer[layer], stabilizer[layer])
        cells.append(new_cell)
        norms.append(new_norm)
        stabs.append(new_stab)
    return (current, jnp.stack(cells), jnp.stack(norms), jnp.stack(stabs))
```

```python
import jax
import jax.numpy as jnp
from jax import lax
from jax.sharding import PartitionSpec as P

EPSILON = 1e-06
NEAR = 4


def near_groups(total, size):
    return [[first + i for i in range(size)] for first in range(0, total, size)]


def far_groups(total, stride):
    return [list(range(first, total, stride)) for first in range(stride)]


def shared(block, groups):
    count = len(groups[0])
    copies = jnp.broadcast_to(block[None], (count, *block.shape))
    return lax.all_to_all(copies, "tp", 0, 0, tiled=True, axis_index_groups=groups)


def gathered(block_t):
    total = lax.axis_size("tp")
    columns, batch = block_t.shape
    half = columns // 2
    packed = jnp.concatenate([block_t[:half], block_t[half:]], axis=1)
    far = shared(packed, far_groups(total, NEAR))
    near = shared(far.reshape(-1, 2 * batch), near_groups(total, NEAR))
    near = near.reshape(NEAR, total // NEAR, half, 2, batch)
    return near.transpose(1, 0, 3, 2, 4).reshape(total * columns, batch)


def project(weight, normed_t):
    return lax.dot_general(
        weight, normed_t, (((1,), (0,)), ((), ())), preferred_element_type=jnp.float32
    )


def three_parts(value):
    high = lax.reduce_precision(value, 8, 7)
    middle = lax.reduce_precision(value - high, 8, 7)
    low = lax.reduce_precision(value - high - middle, 8, 7)
    return [part.astype(jnp.bfloat16) for part in (high, middle, low)]


def one_cell(cur_t, own_t, gain, w_query, w_key, w_value, w_outgate, w_gates, bias_forget, w_proj, cell, norm_vec, stab):
    total = lax.axis_size("tp")
    columns = w_query.shape[0]
    head_size = cell.shape[-1]
    heads = stab.shape[-1]
    batch = cur_t.shape[1]
    group = head_size // columns
    head = lax.axis_index("tp") // group
    cur_f = cur_t.astype(jnp.float32)
    scale = lax.rsqrt(jnp.mean(cur_f * cur_f, axis=0, keepdims=True) + EPSILON)
    normed = (cur_f * scale * gain[:, None]).astype(jnp.bfloat16)
    query = project(w_query, normed).astype(jnp.bfloat16)
    keys = (project(w_key, normed) * head_size ** (-0.5)).astype(jnp.bfloat16)
    gates = project(w_gates.T, normed)
    in_gate = gates[:heads]
    log_forget = jax.nn.log_sigmoid(gates[heads:] + bias_forget[:, None])
    stab_t = stab.T
    new_stab = jnp.maximum(log_forget + stab_t, in_gate)
    decay = jnp.exp(log_forget + stab_t - new_stab)
    weight_in = jnp.exp(in_gate - new_stab)
    select = (jnp.arange(heads) == head).astype(jnp.float32)[:, None]
    my_decay = jnp.sum(decay * select, axis=0)
    my_weight = jnp.sum(weight_in * select, axis=0)
    my_stab = jnp.sum(new_stab * select, axis=0)
    new_norm = my_decay[None] * norm_vec.T + my_weight[None] * keys.astype(jnp.float32)
    den_part = jnp.sum(query.astype(jnp.float32) * new_norm, axis=0)
    high, middle, low = three_parts(den_part)
    extra = jnp.concatenate([high, middle, low, jnp.zeros_like(low)]).reshape(2, 2 * batch)
    extra = jnp.concatenate([extra, jnp.zeros((14, 2 * batch), jnp.bfloat16)])
    message = jnp.concatenate([jnp.concatenate([query, keys], axis=1), extra])
    everyone = shared(message, near_groups(total, group))
    q_head = everyone[:, :columns, :batch].reshape(head_size, batch).T
    k_head = everyone[:, :columns, batch:].reshape(head_size, batch).T
    parts = everyone[:, columns : columns + 2].astype(jnp.float32)
    denom = jnp.sum(parts[:, 0, :batch] + parts[:, 0, batch:] + parts[:, 1, :batch], axis=0)
    values = project(w_value, normed).astype(jnp.bfloat16).T
    outgate = project(w_outgate, normed).astype(jnp.bfloat16)
    outer = values.astype(jnp.float32)[:, :, None] * k_head.astype(jnp.float32)[:, None, :]
    new_cell = my_decay[:, None, None] * cell + my_weight[:, None, None] * outer
    numer = jnp.einsum(
        "bk,bek->be", q_head.astype(jnp.float32), new_cell, precision=lax.Precision.HIGHEST
    )
    readout = numer.T / jnp.maximum(jnp.abs(denom), jnp.exp(-my_stab))[None]
    branch = (jax.nn.sigmoid(outgate.astype(jnp.float32)) * readout).astype(jnp.bfloat16)
    summed = project(w_proj, gathered(branch))
    result = (own_t.astype(jnp.float32) + summed).astype(jnp.bfloat16)
    return result, new_cell, new_norm.T, new_stab.T


def body(tokens, norm_gain, query_weight, key_weight, value_weight, outgate_weight, gate_weight, forget_bias, proj_weight, cell_state, normalizer, stabilizer):
    layers = query_weight.shape[0]
    columns = query_weight.shape[1]
    current = tokens.T
    result = lax.dynamic_slice_in_dim(current, lax.axis_index("tp") * columns, columns, 0)
    cells, norms, stabs = [], [], []
    for layer in range(layers):
        result, new_cell, new_norm, new_stab = one_cell(
            current,
            result,
            norm_gain[layer],
            query_weight[layer],
            key_weight[layer],
            value_weight[layer],
            outgate_weight[layer],
            gate_weight[layer],
            forget_bias[layer],
            proj_weight[layer],
            cell_state[layer],
            normalizer[layer],
            stabilizer[layer],
        )
        cells.append(new_cell)
        norms.append(new_norm)
        stabs.append(new_stab)
        if layer + 1 < layers:
            current = gathered(result)
    return (result.T, jnp.stack(cells), jnp.stack(norms), jnp.stack(stabs))


def solution(mesh):
    return jax.shard_map(
        body,
        mesh=mesh,
        in_specs=(
            P("grp", None),
            P(),
            P(None, "tp", None),
            P(None, "tp", None),
            P(None, "tp", None),
            P(None, "tp", None),
            P(),
            P(),
            P(None, "tp", None),
            P(None, "grp", "tp", None),
            P(None, "grp", "tp"),
            P(None, "grp", None),
        ),
        out_specs=(
            P("grp", "tp"),
            P(None, "grp", "tp", None),
            P(None, "grp", "tp"),
            P(None, "grp", None),
        ),
        check_vma=False,
    )
```

```python
import functools

import jax
import jax.numpy as jnp
from jax import lax
from jax.experimental import pallas as pl
from jax.experimental.pallas import tpu as pltpu
from jax.sharding import PartitionSpec as P

EPSILON = 1e-06
NEAR = 4
CHUNKS = 4
UNROLLED = 8
F32 = jnp.float32
BF16 = jnp.bfloat16
LIMITED = pltpu.CompilerParams(vmem_limit_bytes=16 * 2**20)


def near_groups(total, size):
    return [[first + i for i in range(size)] for first in range(0, total, size)]


def far_groups(total, stride):
    return [list(range(first, total, stride)) for first in range(stride)]


def exchanged(copies, groups):
    return lax.all_to_all(copies, "tp", 0, 0, tiled=True, axis_index_groups=groups)


def from_partner(value, mask):
    pairs = [(source, source ^ mask) for source in range(lax.axis_size("tp"))]
    return lax.ppermute(value, "tp", pairs)


def gathered(copies, meanwhile=None):
    count, rows, lanes = copies.shape
    far = exchanged(copies, far_groups(lax.axis_size("tp"), NEAR))
    own = far.reshape(count * rows, lanes)
    second = from_partner(own, 2)
    first = from_partner(own, 1)
    made = None
    if meanwhile is not None:
        second, made = lax.optimization_barrier((second, meanwhile(own)))
    third = from_partner(second, 1)
    return (own, first, second, third), made


def whole(shape):
    return pl.BlockSpec(shape, lambda *_: (0,) * len(shape))


def one_layer(shape, layer):
    return pl.BlockSpec((None, *shape), lambda *_: (layer,) + (0,) * len(shape))


def smem():
    return pl.BlockSpec(memory_space=pltpu.SMEM)


def unpack(place_ref, pieces, stage_ref):
    own = place_ref[1]
    far, per, batch = stage_ref.shape
    half = per // (2 * NEAR)
    for flip, piece in enumerate(pieces):
        start = pl.multiple_of((own ^ flip) * 2 * half, 2 * half)
        both = piece[...].reshape(far, half, 2 * batch)
        stage_ref[:, pl.ds(start, half), :] = both[:, :, :batch]
        stage_ref[:, pl.ds(start + half, half), :] = both[:, :, batch:]


def front_rest(layer, place_ref, outs, bias_ref, stab_ref, norm_ref, message_ref, value_ref, open_ref, rows_ref, new_norm_ref, new_stab_ref, head_size):
    columns, batch = norm_ref.shape
    heads = stab_ref.shape[0]
    head = place_ref[0]
    query = outs[:columns].astype(BF16)
    keys = (outs[columns : 2 * columns] * head_size ** (-0.5)).astype(BF16)
    value_ref[...] = outs[2 * columns : 3 * columns].astype(BF16).astype(F32)
    open_ref[...] = jax.nn.sigmoid(outs[3 * columns : 4 * columns].astype(BF16).astype(F32))
    in_gate = outs[4 * columns : 4 * columns + heads]
    row = lax.broadcasted_iota(jnp.int32, (heads, heads), 0)
    col = lax.broadcasted_iota(jnp.int32, (heads, heads), 1)
    spread = jnp.broadcast_to(bias_ref[layer : layer + 1, :], (heads, heads))
    bias = jnp.sum(jnp.where(row == col, spread, 0.0), axis=1, keepdims=True)
    forget = outs[4 * columns + heads :] + bias
    log_forget = jnp.minimum(forget, 0.0) - jnp.log1p(jnp.exp(-jnp.abs(forget)))
    shifted = log_forget + stab_ref[...]
    new_stab = jnp.maximum(shifted, in_gate)
    decay = jnp.exp(shifted - new_stab)
    weight = jnp.exp(in_gate - new_stab)
    floor = jnp.exp(-new_stab)
    mine = lax.broadcasted_iota(jnp.int32, (heads, batch), 0) == head

    def own(table):
        return jnp.sum(jnp.where(mine, table, 0.0), axis=0, keepdims=True)

    decay, weight, floor = own(decay), own(weight), own(floor)
    new_norm = decay * norm_ref[...] + weight * keys.astype(F32)
    part = jnp.sum(query.astype(F32) * new_norm, axis=0, keepdims=True)
    high = part.astype(BF16).astype(F32)
    middle = (part - high).astype(BF16).astype(F32)
    low = part - high - middle
    none = jnp.zeros_like(low)
    extra = jnp.concatenate(
        [jnp.concatenate([high, middle], axis=1), jnp.concatenate([low, none], axis=1), jnp.zeros((14, 2 * batch), F32)]
    ).astype(BF16)
    message = jnp.concatenate([jnp.concatenate([query, keys], axis=1), extra])
    message_ref[...] = jnp.broadcast_to(message[None], message_ref.shape)
    rows_ref[...] = jnp.concatenate(
        [jnp.concatenate([decay, weight], axis=1), jnp.concatenate([floor, none], axis=1), jnp.zeros((6, 2 * batch), F32)]
    )
    new_norm_ref[...] = new_norm
    new_stab_ref[...] = new_stab


def first_front(place_ref, cell_ref, tokens_ref, gain_ref, wq_ref, wk_ref, wv_ref, wo_ref, wg_ref, *rest, head_size):
    *rest, held_ref, own_ref, arrived = rest
    fetch = pltpu.make_async_copy(cell_ref.at[0], held_ref, arrived)
    fetch.start()
    columns = own_ref.shape[0]
    near = NEAR * columns
    nearby = tokens_ref[:, pl.ds(pl.multiple_of(place_ref[2] * near, near), near)].astype(F32)
    turned = pltpu.roll(nearby, (NEAR - place_ref[1]) % NEAR * columns, 1).T
    own_ref[...] = turned[:columns].astype(BF16)
    current = tokens_ref[...].astype(F32)
    scale = lax.rsqrt(jnp.mean(current * current, axis=1, keepdims=True) + EPSILON)
    normed = (current * scale * gain_ref[0:1, :]).astype(BF16)
    weights = jnp.concatenate([wq_ref[...], wk_ref[...], wv_ref[...], wo_ref[...], wg_ref[...]])
    outs = lax.dot_general(weights, normed, (((1,), (1,)), ((), ())), preferred_element_type=F32)
    front_rest(0, place_ref, outs, *rest, head_size=head_size)
    fetch.wait()


def later_front(place_ref, cell_ref, own_ref, first_ref, second_ref, third_ref, gain_ref, wq_ref, wk_ref, wv_ref, wo_ref, wg_ref, *rest, layer, head_size):
    *rest, held_ref, arrived, stage_ref, normed_ref = rest
    fetch = pltpu.make_async_copy(cell_ref.at[layer], held_ref, arrived)
    fetch.start()
    unpack(place_ref, (own_ref, first_ref, second_ref, third_ref), stage_ref)
    far, per, batch = stage_ref.shape
    current = stage_ref[...].astype(F32)
    square = jnp.sum(jnp.sum(current * current, axis=0), axis=0, keepdims=True)
    scale = lax.rsqrt(square / (far * per) + EPSILON)
    gain = jnp.concatenate([gain_ref[layer : layer + 1, i * per : (i + 1) * per] for i in range(far)]).T
    for i in range(far):
        normed_ref[i * per : (i + 1) * per, :] = (current[i] * scale * gain[:, i : i + 1]).astype(BF16)
    weights = jnp.concatenate([wq_ref[...], wk_ref[...], wv_ref[...], wo_ref[...], wg_ref[...]])
    outs = jnp.dot(weights, normed_ref[...], preferred_element_type=F32)
    front_rest(layer, place_ref, outs, *rest, head_size=head_size)
    fetch.wait()


def in_hbm(*values):
    return [pltpu.with_memory_space_constraint(value, pltpu.HBM) for value in values]


def front(layer, place, current, norm_gain, projections, gates, bias, stab, norm, cell):
    _, columns, width = projections[0].shape
    heads, batch = stab.shape[1:]
    head_size = cell.shape[-1]
    group = head_size // columns
    far = lax.axis_size("tp") // NEAR
    out_shape = (
        jax.ShapeDtypeStruct((group, columns + 16, 2 * batch), BF16),
        jax.ShapeDtypeStruct((columns, batch), F32),
        jax.ShapeDtypeStruct((columns, batch), F32),
        jax.ShapeDtypeStruct((8, 2 * batch), F32),
        jax.ShapeDtypeStruct((columns, batch), F32),
        jax.ShapeDtypeStruct((heads, batch), F32),
        jax.ShapeDtypeStruct(cell.shape[1:], F32),
    )
    out_specs = [whole(out.shape) for out in out_shape[:-1]] + [pl.BlockSpec(memory_space=pl.ANY)]
    tail_specs = [whole(norm_gain.shape)] + [one_layer((columns, width), layer)] * 4 + [
        one_layer((2 * heads, width), layer),
        whole(bias.shape),
        one_layer((heads, batch), layer),
        one_layer((columns, batch), layer),
    ]
    tail = (norm_gain, *projections, gates, bias, stab, norm)
    head_specs = [smem(), pl.BlockSpec(memory_space=pl.ANY)]
    if layer == 0:
        out_shape = (*out_shape, jax.ShapeDtypeStruct((columns, batch), BF16))
        out_specs.append(whole((columns, batch)))
        return pl.pallas_call(
            functools.partial(first_front, head_size=head_size),
            grid=(1,),
            out_shape=out_shape,
            out_specs=out_specs,
            in_specs=head_specs + [whole((batch, width))] + tail_specs,
            scratch_shapes=[pltpu.SemaphoreType.DMA],
            compiler_params=LIMITED,
            name="front_first",
        )(place, *in_hbm(cell, current, *tail))
    per = width // far
    return pl.pallas_call(
        functools.partial(later_front, layer=layer, head_size=head_size),
        grid=(1,),
        out_shape=out_shape,
        out_specs=out_specs,
        in_specs=head_specs + [whole(current[0].shape)] * 4 + tail_specs,
        scratch_shapes=[
            pltpu.SemaphoreType.DMA,
            pltpu.VMEM((far, per, batch), BF16),
            pltpu.VMEM((width, batch), BF16),
        ],
        compiler_params=LIMITED,
        name="front_later",
    )(place, *in_hbm(cell), *current, *tail)


def head_rows(everyone_ref, columns):
    group, _, lanes = everyone_ref.shape
    return everyone_ref[:, :columns, :].astype(F32).reshape(group * columns, lanes)


def read_kernel(everyone_ref, value_ref, open_ref, rows_ref, cell_ref, copies_ref, turned_ref):
    columns, batch = value_ref.shape
    half_keys = cell_ref.shape[2] // 2
    both = head_rows(everyone_ref, columns)
    turned_ref[...] = both.T
    product = jnp.sum(both[:, :batch] * both[:, batch:], axis=0, keepdims=True)
    lane = lax.broadcasted_iota(jnp.int32, (columns, batch), 1)

    def some(step, sums):
        for i in range(UNROLLED):
            b = step * UNROLLED + i
            products = cell_ref[b] * turned_ref[pl.ds(b, 1), :]
            folded = products[:, :half_keys] + products[:, half_keys:]
            sums = jnp.where(lane == b, jnp.sum(folded, axis=1, keepdims=True), sums)
        return sums

    sums = lax.fori_loop(0, batch // UNROLLED, some, jnp.zeros((columns, batch), F32))
    parts = jnp.sum(everyone_ref[:, columns:, :].astype(F32), axis=0)
    denom = parts[0:1, :batch] + parts[0:1, batch:] + parts[1:2, :batch]
    decay = rows_ref[0:1, :batch]
    weight = rows_ref[0:1, batch:]
    floor = rows_ref[1:2, :batch]
    numer = decay * sums + value_ref[...] * (weight * product)
    readout = numer / jnp.maximum(jnp.abs(denom), floor)
    branch = (open_ref[...] * readout).astype(BF16)
    half = columns // 2
    packed = jnp.concatenate([branch[:half], branch[half:]], axis=1)
    copies_ref[...] = jnp.broadcast_to(packed[None], copies_ref.shape)


def read(everyone, value, opened, rows, held):
    columns, batch = value.shape
    far = lax.axis_size("tp") // NEAR
    out_shape = jax.ShapeDtypeStruct((far, columns // 2, 2 * batch), BF16)
    operands = (everyone, value, opened, rows, held)
    return pl.pallas_call(
        read_kernel,
        grid=(1,),
        out_shape=out_shape,
        in_specs=[whole(operand.shape) for operand in operands],
        out_specs=whole(out_shape.shape),
        scratch_shapes=[pltpu.VMEM((2 * batch, held.shape[-1]), F32)],
        compiler_params=LIMITED,
        name="read",
    )(*operands)


def update_kernel(layers, *refs):
    everyone_refs, value_refs, rows_refs, held_refs, norm_refs, stab_refs = (
        refs[k * layers : (k + 1) * layers] for k in range(6)
    )
    _, cell_ref, norms_ref, stabs_ref, turned_ref, decay_ref, added_ref = refs[6 * layers :]
    step = pl.program_id(0) % CHUNKS
    chunk, columns, keys = cell_ref.shape
    batch = added_ref.shape[1] // 2

    def one(layer):
        @pl.when(step == 0)
        def _():
            rows = rows_refs[layer]
            turned_ref[...] = head_rows(everyone_refs[layer], columns).T
            decay_ref[...] = jnp.broadcast_to(rows[0:1, :], (2 * batch, 2 * batch)).T
            scaled = value_refs[layer][...] * rows[0:1, batch:]
            added_ref[...] = jnp.concatenate([scaled, scaled], axis=1)
            norms_ref[layer] = norm_refs[layer][...]
            stabs_ref[layer] = stab_refs[layer][...]

        added = pltpu.roll(added_ref[...], batch - step * chunk, 1)
        for i in range(chunk):
            b = step * chunk + i
            key = turned_ref[pl.ds(batch + b, 1), :]
            decay = decay_ref[pl.ds(b, 1), :]
            decay = jnp.concatenate([decay] * (keys // decay.shape[1]), axis=1)
            cell_ref[i] = decay * held_refs[layer][i] + added[:, i : i + 1] * key

    for layer in range(layers):
        pl.when(pl.program_id(0) // CHUNKS == layer)(functools.partial(one, layer))


def update(memory, after):
    layers = len(memory)
    everyone, value, rows, held, norm, stab = zip(*memory)
    columns, batch = value[0].shape
    keys = held[0].shape[-1]
    chunk = batch // CHUNKS
    out_shape = (
        jax.ShapeDtypeStruct((layers, *held[0].shape), F32),
        jax.ShapeDtypeStruct((layers, *norm[0].shape), F32),
        jax.ShapeDtypeStruct((layers, *stab[0].shape), F32),
    )

    def held_spec(layer):
        return pl.BlockSpec((chunk, columns, keys), lambda i: (jnp.clip(i - layer * CHUNKS, 0, CHUNKS - 1), 0, 0))

    def wholes(values):
        return [whole(each.shape) for each in values]

    return pl.pallas_call(
        functools.partial(update_kernel, layers),
        grid=(layers * CHUNKS,),
        out_shape=out_shape,
        in_specs=wholes(everyone)
        + wholes(value)
        + wholes(rows)
        + [held_spec(layer) for layer in range(layers)]
        + wholes(norm)
        + wholes(stab)
        + [pl.BlockSpec(memory_space=pl.ANY)],
        out_specs=(
            pl.BlockSpec((None, chunk, columns, keys), lambda i: (i // CHUNKS, i % CHUNKS, 0, 0)),
            whole(out_shape[1].shape),
            whole(out_shape[2].shape),
        ),
        scratch_shapes=[
            pltpu.VMEM((2 * batch, keys), F32),
            pltpu.VMEM((2 * batch, 2 * batch), F32),
            pltpu.VMEM((columns, 2 * batch), F32),
        ],
        compiler_params=LIMITED,
        name="update",
    )(*everyone, *value, *rows, *held, *norm, *stab, after)


def proj_result(place_ref, pieces, weight_ref, residual_ref, stage_ref):
    unpack(place_ref, pieces, stage_ref)
    far, per, batch = stage_ref.shape
    summed = jnp.dot(weight_ref[...], stage_ref[...].reshape(far * per, batch), preferred_element_type=F32)
    return (residual_ref[...].astype(F32) + summed).astype(BF16)


def proj_kernel(place_ref, own_ref, first_ref, second_ref, third_ref, weight_ref, residual_ref, result_ref, *rest):
    *copies, stage_ref = rest
    pieces = (own_ref, first_ref, second_ref, third_ref)
    result = proj_result(place_ref, pieces, weight_ref, residual_ref, stage_ref)
    result_ref[...] = result
    half = result.shape[0] // 2
    for copies_ref in copies:
        packed = jnp.concatenate([result[:half], result[half:]], axis=1)
        copies_ref[...] = jnp.broadcast_to(packed[None], copies_ref.shape)


def proj(layer, place, pieces, weight, residual, send):
    _, columns, width = weight.shape
    batch = residual.shape[1]
    far = lax.axis_size("tp") // NEAR
    out_shape = [jax.ShapeDtypeStruct((columns, batch), BF16)]
    operands = [place, *pieces, weight, residual]
    in_specs = [smem()] + [whole(pieces[0].shape)] * 4 + [one_layer((columns, width), layer), whole(residual.shape)]
    if send:
        out_shape.append(jax.ShapeDtypeStruct((far, columns // 2, 2 * batch), BF16))
    return pl.pallas_call(
        proj_kernel,
        grid=(1,),
        out_shape=out_shape,
        out_specs=[whole(out.shape) for out in out_shape],
        in_specs=in_specs,
        scratch_shapes=[pltpu.VMEM((far, width // far, batch), BF16)],
        compiler_params=LIMITED,
        name="proj",
    )(*operands)


def body(tokens, norm_gain, query_weight, key_weight, value_weight, outgate_weight, gate_weight, forget_bias, proj_weight, cell_state, normalizer, stabilizer):
    layers, columns, _ = query_weight.shape
    head_size = cell_state.shape[-1]
    group = head_size // columns
    device = lax.axis_index("tp")
    place = jnp.stack([device // group, device % NEAR, device // NEAR]).astype(jnp.int32)
    gates = gate_weight.transpose(0, 2, 1)
    stab = stabilizer.transpose(0, 2, 1)
    norm = normalizer.transpose(0, 2, 1)
    projections = (query_weight, key_weight, value_weight, outgate_weight)
    residual = None
    current = tokens
    memory = []
    for layer in range(layers):
        message, value, opened, rows, new_norm, new_stab, held, *own_input = front(
            layer, place, current, norm_gain, projections, gates, forget_bias, stab, norm, cell_state
        )
        residual = own_input[0] if own_input else residual
        everyone = exchanged(message, near_groups(lax.axis_size("tp"), group))
        copies = read(everyone, value, opened, rows, held)
        memory.append((everyone, value, rows, held, new_norm, new_stab))
        last = layer + 1 == layers
        pieces, states = gathered(copies, functools.partial(update, memory) if last else None)
        residual, *copies = proj(layer, place, pieces, proj_weight, residual, not last)
        if not last:
            current, _ = gathered(copies[0])
    cells, norms, stabs = states
    return (residual.T, cells, norms.transpose(0, 2, 1), stabs.transpose(0, 2, 1))


def solution(mesh):
    return jax.shard_map(
        body,
        mesh=mesh,
        in_specs=(
            P("grp", None),
            P(),
            P(None, "tp", None),
            P(None, "tp", None),
            P(None, "tp", None),
            P(None, "tp", None),
            P(),
            P(),
            P(None, "tp", None),
            P(None, "grp", "tp", None),
            P(None, "grp", "tp"),
            P(None, "grp", None),
        ),
        out_specs=(
            P("grp", "tp"),
            P(None, "grp", "tp", None),
            P(None, "grp", "tp"),
            P(None, "grp", None),
        ),
        check_vma=False,
    )
```

```python
import functools

import jax
import jax.numpy as jnp
from jax import lax
from jax.experimental import pallas as pl
from jax.experimental.pallas import tpu as pltpu
from jax.sharding import PartitionSpec as P

EPSILON = 1e-06
NEAR = 4
CHUNKS = 4
UNROLLED = 8
PIECES = 8
F32 = jnp.float32
BF16 = jnp.bfloat16
LIMITED = pltpu.CompilerParams(vmem_limit_bytes=16 * 2**20)


def near_groups(total, size):
    return [[first + i for i in range(size)] for first in range(0, total, size)]


def far_groups(total, stride):
    return [list(range(first, total, stride)) for first in range(stride)]


def exchanged(copies, groups):
    return lax.all_to_all(copies, "tp", 0, 0, tiled=True, axis_index_groups=groups)


def from_partner(value, mask):
    pairs = [(source, source ^ mask) for source in range(lax.axis_size("tp"))]
    return lax.ppermute(value, "tp", pairs)


def gathered(copies, meanwhile=None):
    count, rows, lanes = copies.shape
    far = exchanged(copies, far_groups(lax.axis_size("tp"), NEAR))
    own = far.reshape(count * rows, lanes)
    second = from_partner(own, 2)
    first = from_partner(own, 1)
    made = None
    if meanwhile is not None:
        second, made = lax.optimization_barrier((second, meanwhile(own)))
    third = from_partner(second, 1)
    return (own, first, second, third), made


def whole(shape):
    return pl.BlockSpec(shape, lambda *_: (0,) * len(shape))


def one_layer(shape, layer):
    return pl.BlockSpec((None, *shape), lambda *_: (layer,) + (0,) * len(shape))


def anywhere():
    return pl.BlockSpec(memory_space=pl.ANY)


def smem():
    return pl.BlockSpec(memory_space=pltpu.SMEM)


def unpack(place_ref, pieces, stage_ref):
    own = place_ref[1]
    far, per, batch = stage_ref.shape
    half = per // (2 * NEAR)
    for flip, piece in enumerate(pieces):
        start = pl.multiple_of((own ^ flip) * 2 * half, 2 * half)
        both = piece[...].reshape(far, half, 2 * batch)
        stage_ref[:, pl.ds(start, half), :] = both[:, :, :batch]
        stage_ref[:, pl.ds(start + half, half), :] = both[:, :, batch:]


def front_rest(layer, place_ref, outs, bias_ref, stab_ref, norm_ref, message_ref, value_ref, open_ref, rows_ref, new_norm_ref, new_stab_ref, head_size):
    columns, batch = norm_ref.shape
    heads = stab_ref.shape[0]
    head = place_ref[0]
    query = outs[:columns].astype(BF16)
    keys = (outs[columns : 2 * columns] * head_size ** (-0.5)).astype(BF16)
    value_ref[...] = outs[2 * columns : 3 * columns].astype(BF16).astype(F32)
    open_ref[...] = jax.nn.sigmoid(outs[3 * columns : 4 * columns].astype(BF16).astype(F32))
    in_gate = outs[4 * columns : 4 * columns + heads]
    row = lax.broadcasted_iota(jnp.int32, (heads, heads), 0)
    col = lax.broadcasted_iota(jnp.int32, (heads, heads), 1)
    spread = jnp.broadcast_to(bias_ref[layer : layer + 1, :], (heads, heads))
    bias = jnp.sum(jnp.where(row == col, spread, 0.0), axis=1, keepdims=True)
    forget = outs[4 * columns + heads :] + bias
    log_forget = jnp.minimum(forget, 0.0) - jnp.log1p(jnp.exp(-jnp.abs(forget)))
    shifted = log_forget + stab_ref[...]
    new_stab = jnp.maximum(shifted, in_gate)
    decay = jnp.exp(shifted - new_stab)
    weight = jnp.exp(in_gate - new_stab)
    floor = jnp.exp(-new_stab)
    mine = lax.broadcasted_iota(jnp.int32, (heads, batch), 0) == head

    def own(table):
        return jnp.sum(jnp.where(mine, table, 0.0), axis=0, keepdims=True)

    decay, weight, floor = own(decay), own(weight), own(floor)
    new_norm = decay * norm_ref[...] + weight * keys.astype(F32)
    part = jnp.sum(query.astype(F32) * new_norm, axis=0, keepdims=True)
    high = part.astype(BF16).astype(F32)
    middle = (part - high).astype(BF16).astype(F32)
    low = part - high - middle
    none = jnp.zeros_like(low)
    extra = jnp.concatenate(
        [jnp.concatenate([high, middle], axis=1), jnp.concatenate([low, none], axis=1), jnp.zeros((14, 2 * batch), F32)]
    ).astype(BF16)
    message = jnp.concatenate([jnp.concatenate([query, keys], axis=1), extra])
    message_ref[...] = jnp.broadcast_to(message[None], message_ref.shape)
    rows_ref[...] = jnp.concatenate(
        [jnp.concatenate([decay, weight], axis=1), jnp.concatenate([floor, none], axis=1), jnp.zeros((6, 2 * batch), F32)]
    )
    new_norm_ref[...] = new_norm
    new_stab_ref[...] = new_stab


def fetched(source_ref, target_ref, arrived, pieces):
    size = target_ref.shape[0] // pieces
    return [
        pltpu.make_async_copy(source_ref.at[pl.ds(k * size, size)], target_ref.at[pl.ds(k * size, size)], arrived.at[k])
        for k in range(pieces)
    ]


def first_front(
    place_ref, cell_ref, tokens_hbm, gain_hbm, wq_hbm, wk_hbm, wv_hbm, wo_hbm, wg_hbm, bias_hbm, stab_hbm, norm_hbm, *rest, head_size
):
    *outs, held_ref, own_ref, arrived, loaded, tokens_ref, gain_ref, weights_ref, bias_ref, stab_ref, norm_ref = rest
    columns = own_ref.shape[0]
    gates = wg_hbm.shape[1]
    sources = [tokens_hbm, gain_hbm, bias_hbm, stab_hbm.at[0], norm_hbm.at[0]]
    targets = [tokens_ref, gain_ref, bias_ref, stab_ref, norm_ref]
    for k, weight in enumerate((wq_hbm, wk_hbm, wv_hbm, wo_hbm)):
        sources.append(weight.at[0])
        targets.append(weights_ref.at[pl.ds(k * columns, columns)])
    sources.append(wg_hbm.at[0])
    targets.append(weights_ref.at[pl.ds(4 * columns, gates)])
    loads = [pltpu.make_async_copy(a, b, loaded.at[k]) for k, (a, b) in enumerate(zip(sources, targets))]
    for load in loads:
        load.start()
    fetches = fetched(cell_ref.at[0], held_ref, arrived, PIECES)
    for fetch in fetches:
        fetch.start()
    loads[0].wait()
    loads[1].wait()
    near = NEAR * columns
    nearby = tokens_ref[:, pl.ds(pl.multiple_of(place_ref[2] * near, near), near)].astype(F32)
    turned = pltpu.roll(nearby, (NEAR - place_ref[1]) % NEAR * columns, 1).T
    own_ref[...] = turned[:columns].astype(BF16)
    current = tokens_ref[...].astype(F32)
    scale = lax.rsqrt(jnp.mean(current * current, axis=1, keepdims=True) + EPSILON)
    normed = (current * scale * gain_ref[0:1, :]).astype(BF16)
    for load in loads[2:]:
        load.wait()
    dots = lax.dot_general(weights_ref[...], normed, (((1,), (1,)), ((), ())), preferred_element_type=F32)
    front_rest(0, place_ref, dots, bias_ref, stab_ref, norm_ref, *outs, head_size=head_size)
    for fetch in fetches:
        fetch.wait()


def later_front(place_ref, own_ref, first_ref, second_ref, third_ref, gain_ref, wq_ref, wk_ref, wv_ref, wo_ref, wg_ref, *rest, layer, head_size):
    *rest, stage_ref, normed_ref = rest
    unpack(place_ref, (own_ref, first_ref, second_ref, third_ref), stage_ref)
    far, per, batch = stage_ref.shape
    current = stage_ref[...].astype(F32)
    square = jnp.sum(jnp.sum(current * current, axis=0), axis=0, keepdims=True)
    scale = lax.rsqrt(square / (far * per) + EPSILON)
    gain = jnp.concatenate([gain_ref[layer : layer + 1, i * per : (i + 1) * per] for i in range(far)]).T
    for i in range(far):
        normed_ref[i * per : (i + 1) * per, :] = (current[i] * scale * gain[:, i : i + 1]).astype(BF16)
    weights = jnp.concatenate([wq_ref[...], wk_ref[...], wv_ref[...], wo_ref[...], wg_ref[...]])
    outs = jnp.dot(weights, normed_ref[...], preferred_element_type=F32)
    front_rest(layer, place_ref, outs, *rest, head_size=head_size)


def in_hbm(*values):
    return [pltpu.with_memory_space_constraint(value, pltpu.HBM) for value in values]


def fetch_kernel(layer, cell_ref, after_ref, held_ref, arrived):
    del after_ref
    fetches = fetched(cell_ref.at[layer], held_ref, arrived, PIECES)
    for fetch in fetches:
        fetch.start()
    for fetch in fetches:
        fetch.wait()


def fetch(layer, cell, after):
    return pl.pallas_call(
        functools.partial(fetch_kernel, layer),
        out_shape=jax.ShapeDtypeStruct(cell.shape[1:], F32),
        in_specs=[anywhere()] * 2,
        out_specs=anywhere(),
        scratch_shapes=[pltpu.SemaphoreType.DMA((PIECES,))],
        compiler_params=LIMITED,
        name="fetch",
    )(*in_hbm(cell), after)


def front(layer, place, current, norm_gain, projections, gates, bias, stab, norm, cell):
    _, columns, width = projections[0].shape
    heads, batch = stab.shape[1:]
    head_size = cell.shape[-1]
    group = head_size // columns
    far = lax.axis_size("tp") // NEAR
    out_shape = [
        jax.ShapeDtypeStruct((group, columns + 16, 2 * batch), BF16),
        jax.ShapeDtypeStruct((columns, batch), F32),
        jax.ShapeDtypeStruct((columns, batch), F32),
        jax.ShapeDtypeStruct((8, 2 * batch), F32),
        jax.ShapeDtypeStruct((columns, batch), F32),
        jax.ShapeDtypeStruct((heads, batch), F32),
    ]
    out_specs = [whole(out.shape) for out in out_shape]
    if layer == 0:
        operands = (cell, current, norm_gain, *projections, gates, bias, stab, norm)
        return pl.pallas_call(
            functools.partial(first_front, head_size=head_size),
            grid=(1,),
            out_shape=out_shape + [jax.ShapeDtypeStruct(cell.shape[1:], F32), jax.ShapeDtypeStruct((columns, batch), BF16)],
            out_specs=out_specs + [anywhere(), whole((columns, batch))],
            in_specs=[smem()] + [anywhere()] * len(operands),
            scratch_shapes=[
                pltpu.SemaphoreType.DMA((PIECES,)),
                pltpu.SemaphoreType.DMA((10,)),
                pltpu.VMEM((batch, width), BF16),
                pltpu.VMEM(norm_gain.shape, F32),
                pltpu.VMEM((4 * columns + 2 * heads, width), BF16),
                pltpu.VMEM(bias.shape, F32),
                pltpu.VMEM((heads, batch), F32),
                pltpu.VMEM((columns, batch), F32),
            ],
            compiler_params=LIMITED,
            name="front_first",
        )(place, *in_hbm(*operands))
    per = width // far
    return pl.pallas_call(
        functools.partial(later_front, layer=layer, head_size=head_size),
        grid=(1,),
        out_shape=out_shape,
        out_specs=out_specs,
        in_specs=[smem()]
        + [whole(current[0].shape)] * 4
        + [whole(norm_gain.shape)]
        + [one_layer((columns, width), layer)] * 4
        + [
            one_layer((2 * heads, width), layer),
            whole(bias.shape),
            one_layer((heads, batch), layer),
            one_layer((columns, batch), layer),
        ],
        scratch_shapes=[
            pltpu.VMEM((far, per, batch), BF16),
            pltpu.VMEM((width, batch), BF16),
        ],
        compiler_params=LIMITED,
        name="front_later",
    )(place, *current, norm_gain, *projections, gates, bias, stab, norm)


def head_rows(everyone_ref, columns):
    group, _, lanes = everyone_ref.shape
    return everyone_ref[:, :columns, :].astype(F32).reshape(group * columns, lanes)


def read_kernel(everyone_ref, value_ref, open_ref, rows_ref, cell_ref, copies_ref, turned_ref):
    columns, batch = value_ref.shape
    half_keys = cell_ref.shape[2] // 2
    both = head_rows(everyone_ref, columns)
    turned_ref[...] = both.T
    product = jnp.sum(both[:, :batch] * both[:, batch:], axis=0, keepdims=True)
    lane = lax.broadcasted_iota(jnp.int32, (columns, batch), 1)

    def some(step, sums):
        for i in range(UNROLLED):
            b = step * UNROLLED + i
            products = cell_ref[b] * turned_ref[pl.ds(b, 1), :]
            folded = products[:, :half_keys] + products[:, half_keys:]
            sums = jnp.where(lane == b, jnp.sum(folded, axis=1, keepdims=True), sums)
        return sums

    sums = lax.fori_loop(0, batch // UNROLLED, some, jnp.zeros((columns, batch), F32))
    parts = jnp.sum(everyone_ref[:, columns:, :].astype(F32), axis=0)
    denom = parts[0:1, :batch] + parts[0:1, batch:] + parts[1:2, :batch]
    decay = rows_ref[0:1, :batch]
    weight = rows_ref[0:1, batch:]
    floor = rows_ref[1:2, :batch]
    numer = decay * sums + value_ref[...] * (weight * product)
    readout = numer / jnp.maximum(jnp.abs(denom), floor)
    branch = (open_ref[...] * readout).astype(BF16)
    half = columns // 2
    packed = jnp.concatenate([branch[:half], branch[half:]], axis=1)
    copies_ref[...] = jnp.broadcast_to(packed[None], copies_ref.shape)


def read(everyone, value, opened, rows, held):
    columns, batch = value.shape
    far = lax.axis_size("tp") // NEAR
    out_shape = jax.ShapeDtypeStruct((far, columns // 2, 2 * batch), BF16)
    operands = (everyone, value, opened, rows, held)
    return pl.pallas_call(
        read_kernel,
        grid=(1,),
        out_shape=out_shape,
        in_specs=[whole(operand.shape) for operand in operands],
        out_specs=whole(out_shape.shape),
        scratch_shapes=[pltpu.VMEM((2 * batch, held.shape[-1]), F32)],
        compiler_params=LIMITED,
        name="read",
    )(*operands)


def update_kernel(everyone_ref, value_ref, rows_ref, held_ref, *rest):
    *small, cell_ref, turned_ref, decay_ref, added_ref = rest
    step = pl.program_id(0)
    chunk, columns, keys = cell_ref.shape
    batch = added_ref.shape[1] // 2

    @pl.when(step == 0)
    def _():
        turned_ref[...] = head_rows(everyone_ref, columns).T
        decay_ref[...] = jnp.broadcast_to(rows_ref[0:1, :], (2 * batch, 2 * batch)).T
        scaled = value_ref[...] * rows_ref[0:1, batch:]
        added_ref[...] = jnp.concatenate([scaled, scaled], axis=1)

    added = pltpu.roll(added_ref[...], batch - step * chunk, 1)
    for i in range(chunk):
        b = step * chunk + i
        key = turned_ref[pl.ds(batch + b, 1), :]
        decay = decay_ref[pl.ds(b, 1), :]
        decay = jnp.concatenate([decay] * (keys // decay.shape[1]), axis=1)
        cell_ref[i] = decay * held_ref[i] + added[:, i : i + 1] * key


def update(layer, layers, everyone, value, rows, held, into, after):
    columns, batch = value.shape
    keys = held.shape[-1]
    chunk = batch // CHUNKS
    operands = [everyone, value, rows, held, after]
    in_specs = [
        whole(everyone.shape),
        whole(value.shape),
        whole(rows.shape),
        pl.BlockSpec((chunk, columns, keys), lambda i: (i, 0, 0)),
        anywhere(),
    ]
    aliases = {}
    if into is not None:
        operands.extend(in_hbm(into))
        in_specs.append(anywhere())
        aliases = {5: 0}
    return pl.pallas_call(
        update_kernel,
        grid=(CHUNKS,),
        out_shape=jax.ShapeDtypeStruct((layers, *held.shape), F32),
        in_specs=in_specs,
        out_specs=pl.BlockSpec((None, chunk, columns, keys), lambda i: (layer, i, 0, 0)),
        scratch_shapes=[
            pltpu.VMEM((2 * batch, keys), F32),
            pltpu.VMEM((2 * batch, 2 * batch), F32),
            pltpu.VMEM((columns, 2 * batch), F32),
        ],
        input_output_aliases=aliases,
        compiler_params=LIMITED,
        name="update",
    )(*operands)


def stack_kernel(layers, *refs):
    for layer in range(layers):
        refs[-2][layer] = refs[layer][...]
        refs[-1][layer] = refs[layers + layer][...]


def stacked(norms, stabs):
    layers = len(norms)
    out_shape = [jax.ShapeDtypeStruct((layers, *each[0].shape), F32) for each in (norms, stabs)]
    return pl.pallas_call(
        functools.partial(stack_kernel, layers),
        grid=(1,),
        out_shape=out_shape,
        in_specs=[whole(each.shape) for each in (*norms, *stabs)],
        out_specs=[whole(out.shape) for out in out_shape],
        compiler_params=LIMITED,
        name="stack",
    )(*norms, *stabs)


def proj_result(place_ref, pieces, weight_ref, residual_ref, stage_ref):
    unpack(place_ref, pieces, stage_ref)
    far, per, batch = stage_ref.shape
    summed = jnp.dot(weight_ref[...], stage_ref[...].reshape(far * per, batch), preferred_element_type=F32)
    return (residual_ref[...].astype(F32) + summed).astype(BF16)


def proj_kernel(place_ref, own_ref, first_ref, second_ref, third_ref, weight_ref, residual_ref, result_ref, *rest):
    *copies, stage_ref = rest
    pieces = (own_ref, first_ref, second_ref, third_ref)
    result = proj_result(place_ref, pieces, weight_ref, residual_ref, stage_ref)
    result_ref[...] = result
    half = result.shape[0] // 2
    for copies_ref in copies:
        packed = jnp.concatenate([result[:half], result[half:]], axis=1)
        copies_ref[...] = jnp.broadcast_to(packed[None], copies_ref.shape)


def proj(layer, place, pieces, weight, residual, send):
    _, columns, width = weight.shape
    batch = residual.shape[1]
    far = lax.axis_size("tp") // NEAR
    out_shape = [jax.ShapeDtypeStruct((columns, batch), BF16)]
    operands = [place, *pieces, weight, residual]
    in_specs = [smem()] + [whole(pieces[0].shape)] * 4 + [one_layer((columns, width), layer), whole(residual.shape)]
    if send:
        out_shape.append(jax.ShapeDtypeStruct((far, columns // 2, 2 * batch), BF16))
    return pl.pallas_call(
        proj_kernel,
        grid=(1,),
        out_shape=out_shape,
        out_specs=[whole(out.shape) for out in out_shape],
        in_specs=in_specs,
        scratch_shapes=[pltpu.VMEM((far, width // far, batch), BF16)],
        compiler_params=LIMITED,
        name="proj",
    )(*operands)


def body(tokens, norm_gain, query_weight, key_weight, value_weight, outgate_weight, gate_weight, forget_bias, proj_weight, cell_state, normalizer, stabilizer):
    layers, columns, _ = query_weight.shape
    head_size = cell_state.shape[-1]
    group = head_size // columns
    device = lax.axis_index("tp")
    place = jnp.stack([device // group, device % NEAR, device // NEAR]).astype(jnp.int32)
    gates = gate_weight.transpose(0, 2, 1)
    stab = stabilizer.transpose(0, 2, 1)
    norm = normalizer.transpose(0, 2, 1)
    projections = (query_weight, key_weight, value_weight, outgate_weight)
    current = tokens
    cells = None
    held = [None] * layers
    norms, stabs = [], []
    for layer in range(layers):
        last = layer + 1 == layers
        message, value, opened, rows, new_norm, new_stab, *more = front(
            layer, place, current, norm_gain, projections, gates, forget_bias, stab, norm, cell_state
        )
        norms.append(new_norm)
        stabs.append(new_stab)
        if layer == 0:
            held[0], residual = more
        everyone = exchanged(message, near_groups(lax.axis_size("tp"), group))
        copies = read(everyone, value, opened, rows, held[layer])
        write = functools.partial(update, layer, layers, everyone, value, rows, held[layer], cells)
        if last:
            pieces, (cells, small) = gathered(copies, lambda own: (write(own), stacked(norms, stabs)))
            (residual,) = proj(layer, place, pieces, proj_weight, residual, False)
        else:
            pieces, held[layer + 1] = gathered(copies, functools.partial(fetch, layer + 1, cell_state))
            residual, copies = proj(layer, place, pieces, proj_weight, residual, True)
            current, cells = gathered(copies, write)
    return (residual.T, cells, small[0].transpose(0, 2, 1), small[1].transpose(0, 2, 1))


def solution(mesh):
    return jax.shard_map(
        body,
        mesh=mesh,
        in_specs=(
            P("grp", None),
            P(),
            P(None, "tp", None),
            P(None, "tp", None),
            P(None, "tp", None),
            P(None, "tp", None),
            P(),
            P(),
            P(None, "tp", None),
            P(None, "grp", "tp", None),
            P(None, "grp", "tp"),
            P(None, "grp", None),
        ),
        out_specs=(
            P("grp", "tp"),
            P(None, "grp", "tp", None),
            P(None, "grp", "tp"),
            P(None, "grp", None),
        ),
        check_vma=False,
    )
```

```python
import functools

import jax
import jax.numpy as jnp
from jax import lax
from jax.experimental import pallas as pl
from jax.experimental.pallas import tpu as pltpu
from jax.sharding import PartitionSpec as P

EPSILON = 1e-06
NEAR = 4
CHUNKS = 4
UNROLLED = 32
PIECES = 8
F32 = jnp.float32
BF16 = jnp.bfloat16
LIMITED = pltpu.CompilerParams(vmem_limit_bytes=16 * 2**20)


def near_groups(total, size):
    return [[first + i for i in range(size)] for first in range(0, total, size)]


def far_groups(total, stride):
    return [list(range(first, total, stride)) for first in range(stride)]


def exchanged(copies, groups):
    return lax.all_to_all(copies, "tp", 0, 0, tiled=True, axis_index_groups=groups)


def from_partner(value, mask):
    pairs = [(source, source ^ mask) for source in range(lax.axis_size("tp"))]
    return lax.ppermute(value, "tp", pairs)


def gathered(copies, meanwhile=None):
    count, rows, lanes = copies.shape
    far = exchanged(copies, far_groups(lax.axis_size("tp"), NEAR))
    own = far.reshape(count * rows, lanes)
    second = from_partner(own, 2)
    first = from_partner(own, 1)
    made = None
    if meanwhile is not None:
        second, made = lax.optimization_barrier((second, meanwhile(own)))
    third = from_partner(second, 1)
    return (own, first, second, third), made


def whole(shape):
    return pl.BlockSpec(shape, lambda *_: (0,) * len(shape))


def one_layer(shape, layer):
    return pl.BlockSpec((None, *shape), lambda *_: (layer,) + (0,) * len(shape))


def anywhere():
    return pl.BlockSpec(memory_space=pl.ANY)


def near_vmem():
    return pl.BlockSpec(memory_space=pltpu.VMEM)


def unpack(pieces, stage_ref):
    own = lax.axis_index("tp") % NEAR
    far, per, batch = stage_ref.shape
    half = per // (2 * NEAR)
    for flip, piece in enumerate(pieces):
        start = pl.multiple_of((own ^ flip) * 2 * half, 2 * half)
        both = piece[...].reshape(far, half, 2 * batch)
        stage_ref[:, pl.ds(start, half), :] = both[:, :, :batch]
        stage_ref[:, pl.ds(start + half, half), :] = both[:, :, batch:]


def front_rest(layer, outs, bias_ref, stab_ref, norm_ref, message_ref, value_ref, open_ref, rows_ref, new_norm_ref, new_stab_ref, head_size):
    columns, batch = norm_ref.shape
    heads = stab_ref.shape[0]
    head = lax.axis_index("tp") // (head_size // columns)
    query = outs[:columns].astype(BF16)
    keys = (outs[columns : 2 * columns] * head_size ** (-0.5)).astype(BF16)
    value_ref[...] = outs[2 * columns : 3 * columns].astype(BF16).astype(F32)
    open_ref[...] = jax.nn.sigmoid(outs[3 * columns : 4 * columns].astype(BF16).astype(F32))
    in_gate = outs[4 * columns : 4 * columns + heads]
    row = lax.broadcasted_iota(jnp.int32, (heads, heads), 0)
    col = lax.broadcasted_iota(jnp.int32, (heads, heads), 1)
    spread = jnp.broadcast_to(bias_ref[layer : layer + 1, :], (heads, heads))
    bias = jnp.sum(jnp.where(row == col, spread, 0.0), axis=1, keepdims=True)
    forget = outs[4 * columns + heads :] + bias
    log_forget = jnp.minimum(forget, 0.0) - jnp.log1p(jnp.exp(-jnp.abs(forget)))
    shifted = log_forget + stab_ref[...]
    new_stab = jnp.maximum(shifted, in_gate)
    decay = jnp.exp(shifted - new_stab)
    weight = jnp.exp(in_gate - new_stab)
    floor = jnp.exp(-new_stab)
    mine = lax.broadcasted_iota(jnp.int32, (heads, batch), 0) == head

    def own(table):
        return jnp.sum(jnp.where(mine, table, 0.0), axis=0, keepdims=True)

    decay, weight, floor = own(decay), own(weight), own(floor)
    new_norm = decay * norm_ref[...] + weight * keys.astype(F32)
    part = jnp.sum(query.astype(F32) * new_norm, axis=0, keepdims=True)
    high = part.astype(BF16).astype(F32)
    middle = (part - high).astype(BF16).astype(F32)
    low = part - high - middle
    none = jnp.zeros_like(low)
    extra = jnp.concatenate(
        [jnp.concatenate([high, middle], axis=1), jnp.concatenate([low, none], axis=1), jnp.zeros((14, 2 * batch), F32)]
    ).astype(BF16)
    message = jnp.concatenate([jnp.concatenate([query, keys], axis=1), extra])
    message_ref[...] = jnp.broadcast_to(message[None], message_ref.shape)
    rows_ref[...] = jnp.concatenate(
        [jnp.concatenate([decay, weight], axis=1), jnp.concatenate([floor, none], axis=1), jnp.zeros((6, 2 * batch), F32)]
    )
    new_norm_ref[...] = new_norm
    new_stab_ref[...] = new_stab


def fetched(source_ref, target_ref, arrived, pieces):
    size = target_ref.shape[0] // pieces
    return [
        pltpu.make_async_copy(source_ref.at[pl.ds(k * size, size)], target_ref.at[pl.ds(k * size, size)], arrived.at[k])
        for k in range(pieces)
    ]


def first_front(
    cell_ref, tokens_hbm, gain_hbm, wq_hbm, wk_hbm, wv_hbm, wo_hbm, wg_hbm, bias_hbm, stab_hbm, norm_hbm, *rest, head_size
):
    *outs, held_ref, own_ref, arrived, loaded, tokens_ref, gain_ref, weights_ref, bias_ref, stab_ref, norm_ref = rest
    columns = own_ref.shape[0]
    gates = wg_hbm.shape[1]
    sources = [tokens_hbm, gain_hbm, bias_hbm, stab_hbm.at[0], norm_hbm.at[0]]
    targets = [tokens_ref, gain_ref, bias_ref, stab_ref, norm_ref]
    for k, weight in enumerate((wq_hbm, wk_hbm, wv_hbm, wo_hbm)):
        sources.append(weight.at[0])
        targets.append(weights_ref.at[pl.ds(k * columns, columns)])
    sources.append(wg_hbm.at[0])
    targets.append(weights_ref.at[pl.ds(4 * columns, gates)])
    loads = [pltpu.make_async_copy(a, b, loaded.at[k]) for k, (a, b) in enumerate(zip(sources, targets))]
    for load in loads:
        load.start()
    fetches = fetched(cell_ref.at[0], held_ref, arrived, PIECES)
    for fetch in fetches:
        fetch.start()
    loads[0].wait()
    loads[1].wait()
    near = NEAR * columns
    device = lax.axis_index("tp")
    nearby = tokens_ref[:, pl.ds(pl.multiple_of(device // NEAR * near, near), near)].astype(F32)
    turned = pltpu.roll(nearby, (NEAR - device % NEAR) % NEAR * columns, 1).T
    own_ref[...] = turned[:columns].astype(BF16)
    current = tokens_ref[...].astype(F32)
    scale = lax.rsqrt(jnp.mean(current * current, axis=1, keepdims=True) + EPSILON)
    normed = (current * scale * gain_ref[0:1, :]).astype(BF16)
    for load in loads[2:]:
        load.wait()
    dots = lax.dot_general(weights_ref[...], normed, (((1,), (1,)), ((), ())), preferred_element_type=F32)
    front_rest(0, dots, bias_ref, stab_ref, norm_ref, *outs, head_size=head_size)
    for fetch in fetches:
        fetch.wait()


def later_front(own_ref, first_ref, second_ref, third_ref, gain_ref, wq_ref, wk_ref, wv_ref, wo_ref, wg_ref, *rest, layer, head_size):
    *rest, stage_ref, normed_ref = rest
    unpack((own_ref, first_ref, second_ref, third_ref), stage_ref)
    far, per, batch = stage_ref.shape
    current = stage_ref[...].astype(F32)
    square = jnp.sum(jnp.sum(current * current, axis=0), axis=0, keepdims=True)
    scale = lax.rsqrt(square / (far * per) + EPSILON)
    gain = jnp.concatenate([gain_ref[layer : layer + 1, i * per : (i + 1) * per] for i in range(far)]).T
    for i in range(far):
        normed_ref[i * per : (i + 1) * per, :] = (current[i] * scale * gain[:, i : i + 1]).astype(BF16)
    weights = jnp.concatenate([wq_ref[layer], wk_ref[layer], wv_ref[layer], wo_ref[layer], wg_ref[layer]])
    outs = jnp.dot(weights, normed_ref[...], preferred_element_type=F32)
    bias_ref, stab_ref, norm_ref, *made = rest
    front_rest(layer, outs, bias_ref, stab_ref.at[layer], norm_ref.at[layer], *made, head_size=head_size)


def in_hbm(*values):
    return [pltpu.with_memory_space_constraint(value, pltpu.HBM) for value in values]


def fetch_kernel(layer, cell_ref, after_ref, held_ref, arrived):
    del after_ref
    fetches = fetched(cell_ref.at[layer], held_ref, arrived, PIECES)
    for fetch in fetches:
        fetch.start()
    for fetch in fetches:
        fetch.wait()


def fetch(layer, cell, after):
    return pl.pallas_call(
        functools.partial(fetch_kernel, layer),
        out_shape=jax.ShapeDtypeStruct(cell.shape[1:], F32),
        in_specs=[anywhere()] * 2,
        out_specs=anywhere(),
        scratch_shapes=[pltpu.SemaphoreType.DMA((PIECES,))],
        compiler_params=LIMITED,
        name="fetch",
    )(*in_hbm(cell), after)


def front(layer, current, norm_gain, projections, gates, bias, stab, norm, cell):
    _, columns, width = projections[0].shape
    heads, batch = stab.shape[1:]
    head_size = cell.shape[-1]
    group = head_size // columns
    far = lax.axis_size("tp") // NEAR
    out_shape = [
        jax.ShapeDtypeStruct((group, columns + 16, 2 * batch), BF16),
        jax.ShapeDtypeStruct((columns, batch), F32),
        jax.ShapeDtypeStruct((columns, batch), F32),
        jax.ShapeDtypeStruct((8, 2 * batch), F32),
        jax.ShapeDtypeStruct((columns, batch), F32),
        jax.ShapeDtypeStruct((heads, batch), F32),
    ]
    if layer == 0:
        operands = (cell, current, norm_gain, *projections, gates, bias, stab, norm)
        return pl.pallas_call(
            functools.partial(first_front, head_size=head_size),
            out_shape=out_shape + [jax.ShapeDtypeStruct(cell.shape[1:], F32), jax.ShapeDtypeStruct((columns, batch), BF16)],
            out_specs=[near_vmem()] * len(out_shape) + [anywhere(), near_vmem()],
            in_specs=[anywhere()] * len(operands),
            scratch_shapes=[
                pltpu.SemaphoreType.DMA((PIECES,)),
                pltpu.SemaphoreType.DMA((10,)),
                pltpu.VMEM((batch, width), BF16),
                pltpu.VMEM(norm_gain.shape, F32),
                pltpu.VMEM((4 * columns + 2 * heads, width), BF16),
                pltpu.VMEM(bias.shape, F32),
                pltpu.VMEM((heads, batch), F32),
                pltpu.VMEM((columns, batch), F32),
            ],
            compiler_params=LIMITED,
            name="front_first",
        )(*in_hbm(*operands))
    per = width // far
    operands = (*current, norm_gain, *projections, gates, bias, stab, norm)
    return pl.pallas_call(
        functools.partial(later_front, layer=layer, head_size=head_size),
        out_shape=out_shape,
        out_specs=[near_vmem()] * len(out_shape),
        in_specs=[near_vmem()] * len(operands),
        scratch_shapes=[
            pltpu.VMEM((far, per, batch), BF16),
            pltpu.VMEM((width, batch), BF16),
        ],
        compiler_params=LIMITED,
        name="front_later",
    )(*operands)


def head_rows(everyone_ref, columns):
    group, _, lanes = everyone_ref.shape
    return everyone_ref[:, :columns, :].astype(F32).reshape(group * columns, lanes)


def read_kernel(everyone_ref, value_ref, open_ref, rows_ref, cell_ref, copies_ref, turned_ref):
    columns, batch = value_ref.shape
    half_keys = cell_ref.shape[2] // 2
    both = head_rows(everyone_ref, columns)
    turned_ref[...] = both.T
    product = jnp.sum(both[:, :batch] * both[:, batch:], axis=0, keepdims=True)
    lane = lax.broadcasted_iota(jnp.int32, (columns, batch), 1)

    def some(step, sums):
        for i in range(UNROLLED):
            b = step * UNROLLED + i
            products = cell_ref[b] * turned_ref[pl.ds(b, 1), :]
            folded = products[:, :half_keys] + products[:, half_keys:]
            sums = jnp.where(lane == b, jnp.sum(folded, axis=1, keepdims=True), sums)
        return sums

    sums = lax.fori_loop(0, batch // UNROLLED, some, jnp.zeros((columns, batch), F32))
    parts = jnp.sum(everyone_ref[:, columns:, :].astype(F32), axis=0)
    denom = parts[0:1, :batch] + parts[0:1, batch:] + parts[1:2, :batch]
    decay = rows_ref[0:1, :batch]
    weight = rows_ref[0:1, batch:]
    floor = rows_ref[1:2, :batch]
    numer = decay * sums + value_ref[...] * (weight * product)
    readout = numer / jnp.maximum(jnp.abs(denom), floor)
    branch = (open_ref[...] * readout).astype(BF16)
    half = columns // 2
    packed = jnp.concatenate([branch[:half], branch[half:]], axis=1)
    copies_ref[...] = jnp.broadcast_to(packed[None], copies_ref.shape)


def read(everyone, value, opened, rows, held):
    columns, batch = value.shape
    far = lax.axis_size("tp") // NEAR
    out_shape = jax.ShapeDtypeStruct((far, columns // 2, 2 * batch), BF16)
    operands = (everyone, value, opened, rows, held)
    return pl.pallas_call(
        read_kernel,
        out_shape=out_shape,
        in_specs=[near_vmem()] * len(operands),
        out_specs=near_vmem(),
        scratch_shapes=[pltpu.VMEM((2 * batch, held.shape[-1]), F32)],
        compiler_params=LIMITED,
        name="read",
    )(*operands)


def update_kernel(everyone_ref, value_ref, rows_ref, held_ref, *rest):
    *small, cell_ref, turned_ref, decay_ref, added_ref = rest
    step = pl.program_id(0)
    chunk, columns, keys = cell_ref.shape
    batch = added_ref.shape[1] // 2

    @pl.when(step == 0)
    def _():
        turned_ref[...] = head_rows(everyone_ref, columns).T
        decay_ref[...] = jnp.broadcast_to(rows_ref[0:1, :], (2 * batch, 2 * batch)).T
        scaled = value_ref[...] * rows_ref[0:1, batch:]
        added_ref[...] = jnp.concatenate([scaled, scaled], axis=1)

    added = pltpu.roll(added_ref[...], batch - step * chunk, 1)
    for i in range(chunk):
        b = step * chunk + i
        key = turned_ref[pl.ds(batch + b, 1), :]
        decay = decay_ref[pl.ds(b, 1), :]
        decay = jnp.concatenate([decay] * (keys // decay.shape[1]), axis=1)
        cell_ref[i] = decay * held_ref[i] + added[:, i : i + 1] * key


def update(layer, layers, everyone, value, rows, held, into, after):
    columns, batch = value.shape
    keys = held.shape[-1]
    chunk = batch // CHUNKS
    operands = [everyone, value, rows, held, after]
    in_specs = [
        whole(everyone.shape),
        whole(value.shape),
        whole(rows.shape),
        pl.BlockSpec((chunk, columns, keys), lambda i: (i, 0, 0)),
        anywhere(),
    ]
    aliases = {}
    if into is not None:
        operands.extend(in_hbm(into))
        in_specs.append(anywhere())
        aliases = {5: 0}
    return pl.pallas_call(
        update_kernel,
        grid=(CHUNKS,),
        out_shape=jax.ShapeDtypeStruct((layers, *held.shape), F32),
        in_specs=in_specs,
        out_specs=pl.BlockSpec((None, chunk, columns, keys), lambda i: (layer, i, 0, 0)),
        scratch_shapes=[
            pltpu.VMEM((2 * batch, keys), F32),
            pltpu.VMEM((2 * batch, 2 * batch), F32),
            pltpu.VMEM((columns, 2 * batch), F32),
        ],
        input_output_aliases=aliases,
        compiler_params=LIMITED,
        name="update",
    )(*operands)


def stack_kernel(layers, *refs):
    for layer in range(layers):
        refs[-2][layer] = refs[layer][...]
        refs[-1][layer] = refs[layers + layer][...]


def stacked(norms, stabs):
    layers = len(norms)
    out_shape = [jax.ShapeDtypeStruct((layers, *each[0].shape), F32) for each in (norms, stabs)]
    return pl.pallas_call(
        functools.partial(stack_kernel, layers),
        grid=(1,),
        out_shape=out_shape,
        in_specs=[whole(each.shape) for each in (*norms, *stabs)],
        out_specs=[whole(out.shape) for out in out_shape],
        compiler_params=LIMITED,
        name="stack",
    )(*norms, *stabs)


def proj_result(layer, pieces, weight_ref, residual_ref, stage_ref):
    unpack(pieces, stage_ref)
    far, per, batch = stage_ref.shape
    summed = jnp.dot(weight_ref[layer], stage_ref[...].reshape(far * per, batch), preferred_element_type=F32)
    return (residual_ref[...].astype(F32) + summed).astype(BF16)


def proj_kernel(layer, own_ref, first_ref, second_ref, third_ref, weight_ref, residual_ref, result_ref, *rest):
    *copies, stage_ref = rest
    pieces = (own_ref, first_ref, second_ref, third_ref)
    result = proj_result(layer, pieces, weight_ref, residual_ref, stage_ref)
    result_ref[...] = result
    half = result.shape[0] // 2
    for copies_ref in copies:
        packed = jnp.concatenate([result[:half], result[half:]], axis=1)
        copies_ref[...] = jnp.broadcast_to(packed[None], copies_ref.shape)


def proj(layer, pieces, weight, residual, send):
    _, columns, width = weight.shape
    batch = residual.shape[1]
    far = lax.axis_size("tp") // NEAR
    out_shape = [jax.ShapeDtypeStruct((columns, batch), BF16)]
    operands = (*pieces, weight, residual)
    if send:
        out_shape.append(jax.ShapeDtypeStruct((far, columns // 2, 2 * batch), BF16))
    return pl.pallas_call(
        functools.partial(proj_kernel, layer),
        out_shape=out_shape,
        in_specs=[near_vmem()] * len(operands),
        out_specs=[near_vmem()] * len(out_shape),
        scratch_shapes=[pltpu.VMEM((far, width // far, batch), BF16)],
        compiler_params=LIMITED,
        name="proj",
    )(*operands)


def body(tokens, norm_gain, query_weight, key_weight, value_weight, outgate_weight, gate_weight, forget_bias, proj_weight, cell_state, normalizer, stabilizer):
    layers, columns, _ = query_weight.shape
    head_size = cell_state.shape[-1]
    group = head_size // columns
    gates = gate_weight.transpose(0, 2, 1)
    stab = stabilizer.transpose(0, 2, 1)
    norm = normalizer.transpose(0, 2, 1)
    projections = (query_weight, key_weight, value_weight, outgate_weight)
    current = tokens
    cells = None
    held = [None] * layers
    norms, stabs = [], []
    for layer in range(layers):
        last = layer + 1 == layers
        message, value, opened, rows, new_norm, new_stab, *more = front(
            layer, current, norm_gain, projections, gates, forget_bias, stab, norm, cell_state
        )
        norms.append(new_norm)
        stabs.append(new_stab)
        if layer == 0:
            held[0], residual = more
        everyone = exchanged(message, near_groups(lax.axis_size("tp"), group))
        copies = read(everyone, value, opened, rows, held[layer])
        write = functools.partial(update, layer, layers, everyone, value, rows, held[layer], cells)
        if last:
            pieces, (cells, small) = gathered(copies, lambda own: (write(own), stacked(norms, stabs)))
            (residual,) = proj(layer, pieces, proj_weight, residual, False)
        else:
            pieces, held[layer + 1] = gathered(copies, functools.partial(fetch, layer + 1, cell_state))
            residual, copies = proj(layer, pieces, proj_weight, residual, True)
            current, cells = gathered(copies, write)
    return (residual.T, cells, small[0].transpose(0, 2, 1), small[1].transpose(0, 2, 1))


def solution(mesh):
    return jax.shard_map(
        body,
        mesh=mesh,
        in_specs=(
            P("grp", None),
            P(),
            P(None, "tp", None),
            P(None, "tp", None),
            P(None, "tp", None),
            P(None, "tp", None),
            P(),
            P(),
            P(None, "tp", None),
            P(None, "grp", "tp", None),
            P(None, "grp", "tp"),
            P(None, "grp", None),
        ),
        out_specs=(
            P("grp", "tp"),
            P(None, "grp", "tp", None),
            P(None, "grp", "tp"),
            P(None, "grp", None),
        ),
        check_vma=False,
    )
```

```python
import functools

import jax
import jax.numpy as jnp
from jax import lax
from jax.experimental import pallas as pl
from jax.experimental.pallas import tpu as pltpu
from jax.sharding import PartitionSpec as P

EPSILON = 1e-06
NEAR = 4
CHUNKS = 4
UNROLLED = 32
PIECES = 4
F32 = jnp.float32
BF16 = jnp.bfloat16
LIMITED = pltpu.CompilerParams(vmem_limit_bytes=16 * 2**20)


def near_groups(total, size):
    return [[first + i for i in range(size)] for first in range(0, total, size)]


def far_groups(total, stride):
    return [list(range(first, total, stride)) for first in range(stride)]


def exchanged(copies, groups):
    return lax.all_to_all(copies, "tp", 0, 0, tiled=True, axis_index_groups=groups)


def from_partner(value, mask):
    pairs = [(source, source ^ mask) for source in range(lax.axis_size("tp"))]
    return lax.ppermute(value, "tp", pairs)


def gathered(copies, meanwhile=None):
    count, rows, lanes = copies.shape
    far = exchanged(copies, far_groups(lax.axis_size("tp"), NEAR))
    own = far.reshape(count * rows, lanes)
    second = from_partner(own, 2)
    first = from_partner(own, 1)
    made = None
    if meanwhile is not None:
        second, made = lax.optimization_barrier((second, meanwhile(own)))
    third = from_partner(second, 1)
    return (own, first, second, third), made


def whole(shape):
    return pl.BlockSpec(shape, lambda *_: (0,) * len(shape))


def one_layer(shape, layer):
    return pl.BlockSpec((None, *shape), lambda *_: (layer,) + (0,) * len(shape))


def anywhere():
    return pl.BlockSpec(memory_space=pl.ANY)


def near_vmem():
    return pl.BlockSpec(memory_space=pltpu.VMEM)


def unpack(pieces, stage_ref):
    own = lax.axis_index("tp") % NEAR
    far, per, batch = stage_ref.shape
    half = per // (2 * NEAR)
    for flip, piece in enumerate(pieces):
        start = pl.multiple_of((own ^ flip) * 2 * half, 2 * half)
        both = piece[...].reshape(far, half, 2 * batch)
        stage_ref[:, pl.ds(start, half), :] = both[:, :, :batch]
        stage_ref[:, pl.ds(start + half, half), :] = both[:, :, batch:]


def front_rest(layer, outs, bias_ref, stab_ref, norm_ref, message_ref, value_ref, open_ref, rows_ref, new_norm_ref, new_stab_ref, head_size):
    columns, batch = norm_ref.shape
    heads = stab_ref.shape[0]
    head = lax.axis_index("tp") // (head_size // columns)
    query = outs[:columns].astype(BF16)
    keys = (outs[columns : 2 * columns] * head_size ** (-0.5)).astype(BF16)
    value_ref[...] = outs[2 * columns : 3 * columns].astype(BF16).astype(F32)
    open_ref[...] = jax.nn.sigmoid(outs[3 * columns : 4 * columns].astype(BF16).astype(F32))
    in_gate = outs[4 * columns : 4 * columns + heads]
    row = lax.broadcasted_iota(jnp.int32, (heads, heads), 0)
    col = lax.broadcasted_iota(jnp.int32, (heads, heads), 1)
    spread = jnp.broadcast_to(bias_ref[layer : layer + 1, :], (heads, heads))
    bias = jnp.sum(jnp.where(row == col, spread, 0.0), axis=1, keepdims=True)
    forget = outs[4 * columns + heads :] + bias
    log_forget = jnp.minimum(forget, 0.0) - jnp.log1p(jnp.exp(-jnp.abs(forget)))
    shifted = log_forget + stab_ref[...]
    new_stab = jnp.maximum(shifted, in_gate)
    decay = jnp.exp(shifted - new_stab)
    weight = jnp.exp(in_gate - new_stab)
    floor = jnp.exp(-new_stab)
    mine = lax.broadcasted_iota(jnp.int32, (heads, batch), 0) == head

    def own(table):
        return jnp.sum(jnp.where(mine, table, 0.0), axis=0, keepdims=True)

    decay, weight, floor = own(decay), own(weight), own(floor)
    new_norm = decay * norm_ref[...] + weight * keys.astype(F32)
    part = jnp.sum(query.astype(F32) * new_norm, axis=0, keepdims=True)
    high = part.astype(BF16).astype(F32)
    middle = (part - high).astype(BF16).astype(F32)
    low = part - high - middle
    none = jnp.zeros_like(low)
    extra = jnp.concatenate(
        [jnp.concatenate([high, middle], axis=1), jnp.concatenate([low, none], axis=1), jnp.zeros((14, 2 * batch), F32)]
    ).astype(BF16)
    message = jnp.concatenate([jnp.concatenate([query, keys], axis=1), extra])
    message_ref[...] = jnp.broadcast_to(message[None], message_ref.shape)
    rows_ref[...] = jnp.concatenate(
        [jnp.concatenate([decay, weight], axis=1), jnp.concatenate([floor, none], axis=1), jnp.zeros((6, 2 * batch), F32)]
    )
    new_norm_ref[...] = new_norm
    new_stab_ref[...] = new_stab


def fetched(source_ref, target_ref, arrived, pieces):
    size = target_ref.shape[0] // pieces
    return [
        pltpu.make_async_copy(source_ref.at[pl.ds(k * size, size)], target_ref.at[pl.ds(k * size, size)], arrived.at[k])
        for k in range(pieces)
    ]


def first_front(
    cell_ref, tokens_hbm, gain_hbm, wq_hbm, wk_hbm, wv_hbm, wo_hbm, wg_hbm, bias_hbm, stab_hbm, norm_hbm, *rest, head_size
):
    *outs, held_ref, own_ref, arrived, loaded, tokens_ref, gain_ref, weights_ref, bias_ref, stab_ref, norm_ref = rest
    columns = own_ref.shape[0]
    gates = wg_hbm.shape[1]
    sources = [tokens_hbm, gain_hbm, bias_hbm, stab_hbm.at[0], norm_hbm.at[0]]
    targets = [tokens_ref, gain_ref, bias_ref, stab_ref, norm_ref]
    for k, weight in enumerate((wq_hbm, wk_hbm, wv_hbm, wo_hbm)):
        sources.append(weight.at[0])
        targets.append(weights_ref.at[pl.ds(k * columns, columns)])
    sources.append(wg_hbm.at[0])
    targets.append(weights_ref.at[pl.ds(4 * columns, gates)])
    loads = [pltpu.make_async_copy(a, b, loaded.at[k]) for k, (a, b) in enumerate(zip(sources, targets))]
    for load in loads:
        load.start()
    fetches = fetched(cell_ref.at[0], held_ref, arrived, PIECES)
    for fetch in fetches:
        fetch.start()
    loads[0].wait()
    loads[1].wait()
    near = NEAR * columns
    device = lax.axis_index("tp")
    nearby = tokens_ref[:, pl.ds(pl.multiple_of(device // NEAR * near, near), near)].astype(F32)
    turned = pltpu.roll(nearby, (NEAR - device % NEAR) % NEAR * columns, 1).T
    own_ref[...] = turned[:columns].astype(BF16)
    current = tokens_ref[...].astype(F32)
    scale = lax.rsqrt(jnp.mean(current * current, axis=1, keepdims=True) + EPSILON)
    normed = (current * scale * gain_ref[0:1, :]).astype(BF16)
    for load in loads[2:]:
        load.wait()
    dots = lax.dot_general(weights_ref[...], normed, (((1,), (1,)), ((), ())), preferred_element_type=F32)
    front_rest(0, dots, bias_ref, stab_ref, norm_ref, *outs, head_size=head_size)
    for fetch in fetches:
        fetch.wait()


def later_front(own_ref, first_ref, second_ref, third_ref, gain_ref, wq_ref, wk_ref, wv_ref, wo_ref, wg_ref, *rest, layer, head_size):
    *rest, stage_ref, normed_ref = rest
    unpack((own_ref, first_ref, second_ref, third_ref), stage_ref)
    far, per, batch = stage_ref.shape
    current = stage_ref[...].astype(F32)
    square = jnp.sum(jnp.sum(current * current, axis=0), axis=0, keepdims=True)
    scale = lax.rsqrt(square / (far * per) + EPSILON)
    gain = jnp.concatenate([gain_ref[layer : layer + 1, i * per : (i + 1) * per] for i in range(far)]).T
    for i in range(far):
        normed_ref[i * per : (i + 1) * per, :] = (current[i] * scale * gain[:, i : i + 1]).astype(BF16)
    weights = jnp.concatenate([wq_ref[layer], wk_ref[layer], wv_ref[layer], wo_ref[layer], wg_ref[layer]])
    outs = jnp.dot(weights, normed_ref[...], preferred_element_type=F32)
    bias_ref, stab_ref, norm_ref, *made = rest
    front_rest(layer, outs, bias_ref, stab_ref.at[layer], norm_ref.at[layer], *made, head_size=head_size)


def in_hbm(*values):
    return [pltpu.with_memory_space_constraint(value, pltpu.HBM) for value in values]


def fetch_kernel(layer, cell_ref, after_ref, held_ref, arrived):
    del after_ref
    fetches = fetched(cell_ref.at[layer], held_ref, arrived, PIECES)
    for fetch in fetches:
        fetch.start()
    for fetch in fetches:
        fetch.wait()


def fetch(layer, cell, after):
    return pl.pallas_call(
        functools.partial(fetch_kernel, layer),
        out_shape=jax.ShapeDtypeStruct(cell.shape[1:], F32),
        in_specs=[anywhere()] * 2,
        out_specs=anywhere(),
        scratch_shapes=[pltpu.SemaphoreType.DMA((PIECES,))],
        compiler_params=LIMITED,
        name="fetch",
    )(*in_hbm(cell), after)


def front(layer, current, norm_gain, projections, gates, bias, stab, norm, cell):
    _, columns, width = projections[0].shape
    heads, batch = stab.shape[1:]
    head_size = cell.shape[-1]
    group = head_size // columns
    far = lax.axis_size("tp") // NEAR
    out_shape = [
        jax.ShapeDtypeStruct((group, columns + 16, 2 * batch), BF16),
        jax.ShapeDtypeStruct((columns, batch), F32),
        jax.ShapeDtypeStruct((columns, batch), F32),
        jax.ShapeDtypeStruct((8, 2 * batch), F32),
        jax.ShapeDtypeStruct((columns, batch), F32),
        jax.ShapeDtypeStruct((heads, batch), F32),
    ]
    if layer == 0:
        operands = (cell, current, norm_gain, *projections, gates, bias, stab, norm)
        return pl.pallas_call(
            functools.partial(first_front, head_size=head_size),
            out_shape=out_shape + [jax.ShapeDtypeStruct(cell.shape[1:], F32), jax.ShapeDtypeStruct((columns, batch), BF16)],
            out_specs=[near_vmem()] * len(out_shape) + [anywhere(), near_vmem()],
            in_specs=[anywhere()] * len(operands),
            scratch_shapes=[
                pltpu.SemaphoreType.DMA((PIECES,)),
                pltpu.SemaphoreType.DMA((10,)),
                pltpu.VMEM((batch, width), BF16),
                pltpu.VMEM(norm_gain.shape, F32),
                pltpu.VMEM((4 * columns + 2 * heads, width), BF16),
                pltpu.VMEM(bias.shape, F32),
                pltpu.VMEM((heads, batch), F32),
                pltpu.VMEM((columns, batch), F32),
            ],
            compiler_params=LIMITED,
            name="front_first",
        )(*in_hbm(*operands))
    per = width // far
    operands = (*current, norm_gain, *projections, gates, bias, stab, norm)
    return pl.pallas_call(
        functools.partial(later_front, layer=layer, head_size=head_size),
        out_shape=out_shape,
        out_specs=[near_vmem()] * len(out_shape),
        in_specs=[near_vmem()] * len(operands),
        scratch_shapes=[
            pltpu.VMEM((far, per, batch), BF16),
            pltpu.VMEM((width, batch), BF16),
        ],
        compiler_params=LIMITED,
        name="front_later",
    )(*operands)


def head_rows(everyone_ref, columns):
    group, _, lanes = everyone_ref.shape
    return everyone_ref[:, :columns, :].astype(F32).reshape(group * columns, lanes)


def read_kernel(everyone_ref, value_ref, open_ref, rows_ref, cell_ref, copies_ref, turned_ref):
    columns, batch = value_ref.shape
    half_keys = cell_ref.shape[2] // 2
    both = head_rows(everyone_ref, columns)
    turned_ref[...] = both.T
    product = jnp.sum(both[:, :batch] * both[:, batch:], axis=0, keepdims=True)
    lane = lax.broadcasted_iota(jnp.int32, (columns, batch), 1)

    def some(step, sums):
        for i in range(UNROLLED):
            b = step * UNROLLED + i
            products = cell_ref[b] * turned_ref[pl.ds(b, 1), :]
            folded = products[:, :half_keys] + products[:, half_keys:]
            sums = jnp.where(lane == b, jnp.sum(folded, axis=1, keepdims=True), sums)
        return sums

    sums = lax.fori_loop(0, batch // UNROLLED, some, jnp.zeros((columns, batch), F32))
    parts = jnp.sum(everyone_ref[:, columns:, :].astype(F32), axis=0)
    denom = parts[0:1, :batch] + parts[0:1, batch:] + parts[1:2, :batch]
    decay = rows_ref[0:1, :batch]
    weight = rows_ref[0:1, batch:]
    floor = rows_ref[1:2, :batch]
    numer = decay * sums + value_ref[...] * (weight * product)
    readout = numer / jnp.maximum(jnp.abs(denom), floor)
    branch = (open_ref[...] * readout).astype(BF16)
    half = columns // 2
    packed = jnp.concatenate([branch[:half], branch[half:]], axis=1)
    copies_ref[...] = jnp.broadcast_to(packed[None], copies_ref.shape)


def read(everyone, value, opened, rows, held):
    columns, batch = value.shape
    far = lax.axis_size("tp") // NEAR
    out_shape = jax.ShapeDtypeStruct((far, columns // 2, 2 * batch), BF16)
    operands = (everyone, value, opened, rows, held)
    return pl.pallas_call(
        read_kernel,
        out_shape=out_shape,
        in_specs=[near_vmem()] * len(operands),
        out_specs=near_vmem(),
        scratch_shapes=[pltpu.VMEM((2 * batch, held.shape[-1]), F32)],
        compiler_params=LIMITED,
        name="read",
    )(*operands)


def update_kernel(layer, layers, everyone_ref, value_ref, rows_ref, held_ref, *rest):
    *rest, fresh_ref, turned_ref, decay_ref, written = rest
    columns, batch = value_ref.shape
    keys = held_ref.shape[-1]
    if layers:
        norm_refs, stab_refs = rest[:layers], rest[layers : 2 * layers]
        *_, cells_ref, norms_ref, stabs_ref = rest
        for k in range(layers):
            norms_ref[k] = norm_refs[k][...]
            stabs_ref[k] = stab_refs[k][...]
    else:
        cells_ref = rest[-1]
    turned_ref[...] = head_rows(everyone_ref, columns).T
    decay_ref[...] = jnp.broadcast_to(rows_ref[0:1, :], (2 * batch, 2 * batch)).T
    added = value_ref[...] * rows_ref[0:1, batch:]
    chunk = batch // CHUNKS
    writes = []
    for k in range(CHUNKS):
        for b in range(k * chunk, (k + 1) * chunk):
            key = turned_ref[batch + b : batch + b + 1, :]
            decay = decay_ref[b : b + 1, :]
            decay = jnp.concatenate([decay] * (keys // decay.shape[1]), axis=1)
            fresh_ref[b] = decay * held_ref[b] + added[:, b : b + 1] * key
        part = pl.ds(k * chunk, chunk)
        writes.append(pltpu.make_async_copy(fresh_ref.at[part], cells_ref.at[layer, part], written.at[k]))
        writes[-1].start()
    for write in writes:
        write.wait()


def update(layer, layers, everyone, value, rows, held, into, small, after):
    columns, batch = value.shape
    keys = held.shape[-1]
    operands = [everyone, value, rows, held, *small]
    in_specs = [near_vmem()] * len(operands)
    out_shape = [jax.ShapeDtypeStruct((layers, *held.shape), F32)]
    out_specs = [anywhere()]
    if small:
        for each in (small[0], small[-1]):
            out_shape.append(jax.ShapeDtypeStruct((layers, *each.shape), F32))
            out_specs.append(near_vmem())
    operands.append(after)
    in_specs.append(anywhere())
    aliases = {}
    if into is not None:
        aliases = {len(operands): 0}
        operands.extend(in_hbm(into))
        in_specs.append(anywhere())
    return pl.pallas_call(
        functools.partial(update_kernel, layer, len(small) // 2),
        out_shape=out_shape,
        in_specs=in_specs,
        out_specs=out_specs,
        scratch_shapes=[
            pltpu.VMEM(held.shape, F32),
            pltpu.VMEM((2 * batch, keys), F32),
            pltpu.VMEM((2 * batch, 2 * batch), F32),
            pltpu.SemaphoreType.DMA((CHUNKS,)),
        ],
        input_output_aliases=aliases,
        compiler_params=LIMITED,
        name="update",
    )(*operands)


def proj_result(layer, pieces, weight_ref, residual_ref, stage_ref):
    unpack(pieces, stage_ref)
    far, per, batch = stage_ref.shape
    summed = jnp.dot(weight_ref[layer], stage_ref[...].reshape(far * per, batch), preferred_element_type=F32)
    return (residual_ref[...].astype(F32) + summed).astype(BF16)


def proj_kernel(layer, own_ref, first_ref, second_ref, third_ref, weight_ref, residual_ref, result_ref, *rest):
    *copies, stage_ref = rest
    pieces = (own_ref, first_ref, second_ref, third_ref)
    result = proj_result(layer, pieces, weight_ref, residual_ref, stage_ref)
    result_ref[...] = result
    half = result.shape[0] // 2
    for copies_ref in copies:
        packed = jnp.concatenate([result[:half], result[half:]], axis=1)
        copies_ref[...] = jnp.broadcast_to(packed[None], copies_ref.shape)


def proj(layer, pieces, weight, residual, send):
    _, columns, width = weight.shape
    batch = residual.shape[1]
    far = lax.axis_size("tp") // NEAR
    out_shape = [jax.ShapeDtypeStruct((columns, batch), BF16)]
    operands = (*pieces, weight, residual)
    if send:
        out_shape.append(jax.ShapeDtypeStruct((far, columns // 2, 2 * batch), BF16))
    return pl.pallas_call(
        functools.partial(proj_kernel, layer),
        out_shape=out_shape,
        in_specs=[near_vmem()] * len(operands),
        out_specs=[near_vmem()] * len(out_shape),
        scratch_shapes=[pltpu.VMEM((far, width // far, batch), BF16)],
        compiler_params=LIMITED,
        name="proj",
    )(*operands)


def body(tokens, norm_gain, query_weight, key_weight, value_weight, outgate_weight, gate_weight, forget_bias, proj_weight, cell_state, normalizer, stabilizer):
    layers, columns, _ = query_weight.shape
    head_size = cell_state.shape[-1]
    group = head_size // columns
    gates = gate_weight.transpose(0, 2, 1)
    stab = stabilizer.transpose(0, 2, 1)
    norm = normalizer.transpose(0, 2, 1)
    projections = (query_weight, key_weight, value_weight, outgate_weight)
    current = tokens
    cells = None
    held = [None] * layers
    norms, stabs = [], []
    for layer in range(layers):
        last = layer + 1 == layers
        message, value, opened, rows, new_norm, new_stab, *more = front(
            layer, current, norm_gain, projections, gates, forget_bias, stab, norm, cell_state
        )
        norms.append(new_norm)
        stabs.append(new_stab)
        if layer == 0:
            held[0], residual = more
        everyone = exchanged(message, near_groups(lax.axis_size("tp"), group))
        copies = read(everyone, value, opened, rows, held[layer])
        small = (*norms, *stabs) if last else ()
        write = functools.partial(update, layer, layers, everyone, value, rows, held[layer], cells, small)
        if last:
            pieces, states = gathered(copies, write)
            (residual,) = proj(layer, pieces, proj_weight, residual, False)
        else:
            pieces, held[layer + 1] = gathered(copies, functools.partial(fetch, layer + 1, cell_state))
            residual, copies = proj(layer, pieces, proj_weight, residual, True)
            current, (cells,) = gathered(copies, write)
    cells, norms, stabs = states
    return (residual.T, cells, norms.transpose(0, 2, 1), stabs.transpose(0, 2, 1))


def solution(mesh):
    return jax.shard_map(
        body,
        mesh=mesh,
        in_specs=(
            P("grp", None),
            P(),
            P(None, "tp", None),
            P(None, "tp", None),
            P(None, "tp", None),
            P(None, "tp", None),
            P(),
            P(),
            P(None, "tp", None),
            P(None, "grp", "tp", None),
            P(None, "grp", "tp"),
            P(None, "grp", None),
        ),
        out_specs=(
            P("grp", "tp"),
            P(None, "grp", "tp", None),
            P(None, "grp", "tp"),
            P(None, "grp", None),
        ),
        check_vma=False,
    )
```

```python
import functools

import jax
import jax.numpy as jnp
from jax import lax
from jax.experimental import pallas as pl
from jax.experimental.pallas import tpu as pltpu
from jax.sharding import PartitionSpec as P

EPSILON = 1e-06
NEAR = 4
CHUNKS = 4
UNROLLED = 32
PIECES = 4
F32 = jnp.float32
BF16 = jnp.bfloat16
LIMITED = pltpu.CompilerParams(vmem_limit_bytes=16 * 2**20)


def near_groups(total, size):
    return [[first + i for i in range(size)] for first in range(0, total, size)]


def far_groups(total, stride):
    return [list(range(first, total, stride)) for first in range(stride)]


def exchanged(copies, groups):
    return lax.all_to_all(copies, "tp", 0, 0, tiled=True, axis_index_groups=groups)


def from_partner(value, mask):
    pairs = [(source, source ^ mask) for source in range(lax.axis_size("tp"))]
    return lax.ppermute(value, "tp", pairs)


def gathered(copies, meanwhile=None):
    count, rows, lanes = copies.shape
    far = exchanged(copies, far_groups(lax.axis_size("tp"), NEAR))
    own = far.reshape(count * rows, lanes)
    second = from_partner(own, 2)
    third = from_partner(own, 3)
    first = from_partner(own, 1)
    made = None
    if meanwhile is not None:
        first, second, third, made = lax.optimization_barrier((first, second, third, meanwhile(own)))
    return (own, first, second, third), made


def whole(shape):
    return pl.BlockSpec(shape, lambda *_: (0,) * len(shape))


def one_layer(shape, layer):
    return pl.BlockSpec((None, *shape), lambda *_: (layer,) + (0,) * len(shape))


def anywhere():
    return pl.BlockSpec(memory_space=pl.ANY)


def near_vmem():
    return pl.BlockSpec(memory_space=pltpu.VMEM)


def unpack(pieces, stage_ref):
    own = lax.axis_index("tp") % NEAR
    far, per, batch = stage_ref.shape
    half = per // (2 * NEAR)
    for flip, piece in enumerate(pieces):
        start = pl.multiple_of((own ^ flip) * 2 * half, 2 * half)
        both = piece[...].reshape(far, half, 2 * batch)
        stage_ref[:, pl.ds(start, half), :] = both[:, :, :batch]
        stage_ref[:, pl.ds(start + half, half), :] = both[:, :, batch:]


def front_rest(layer, outs, bias_ref, stab_ref, norm_ref, message_ref, value_ref, open_ref, rows_ref, new_norm_ref, new_stab_ref, head_size):
    columns, batch = norm_ref.shape
    heads = stab_ref.shape[0]
    head = lax.axis_index("tp") // (head_size // columns)
    query = outs[:columns].astype(BF16)
    keys = (outs[columns : 2 * columns] * head_size ** (-0.5)).astype(BF16)
    value_ref[...] = outs[2 * columns : 3 * columns].astype(BF16).astype(F32)
    open_ref[...] = jax.nn.sigmoid(outs[3 * columns : 4 * columns].astype(BF16).astype(F32))
    in_gate = outs[4 * columns : 4 * columns + heads]
    row = lax.broadcasted_iota(jnp.int32, (heads, heads), 0)
    col = lax.broadcasted_iota(jnp.int32, (heads, heads), 1)
    spread = jnp.broadcast_to(bias_ref[layer : layer + 1, :], (heads, heads))
    bias = jnp.sum(jnp.where(row == col, spread, 0.0), axis=1, keepdims=True)
    forget = outs[4 * columns + heads :] + bias
    log_forget = jnp.minimum(forget, 0.0) - jnp.log1p(jnp.exp(-jnp.abs(forget)))
    shifted = log_forget + stab_ref[...]
    new_stab = jnp.maximum(shifted, in_gate)
    decay = jnp.exp(shifted - new_stab)
    weight = jnp.exp(in_gate - new_stab)
    floor = jnp.exp(-new_stab)
    mine = lax.broadcasted_iota(jnp.int32, (heads, batch), 0) == head

    def own(table):
        return jnp.sum(jnp.where(mine, table, 0.0), axis=0, keepdims=True)

    decay, weight, floor = own(decay), own(weight), own(floor)
    new_norm = decay * norm_ref[...] + weight * keys.astype(F32)
    part = jnp.sum(query.astype(F32) * new_norm, axis=0, keepdims=True)
    high = part.astype(BF16).astype(F32)
    middle = (part - high).astype(BF16).astype(F32)
    low = part - high - middle
    none = jnp.zeros_like(low)
    extra = jnp.concatenate(
        [jnp.concatenate([high, middle], axis=1), jnp.concatenate([low, none], axis=1), jnp.zeros((14, 2 * batch), F32)]
    ).astype(BF16)
    message = jnp.concatenate([jnp.concatenate([query, keys], axis=1), extra])
    message_ref[...] = jnp.broadcast_to(message[None], message_ref.shape)
    rows_ref[...] = jnp.concatenate(
        [jnp.concatenate([decay, weight], axis=1), jnp.concatenate([floor, none], axis=1), jnp.zeros((6, 2 * batch), F32)]
    )
    new_norm_ref[...] = new_norm
    new_stab_ref[...] = new_stab


def fetched(source_ref, target_ref, arrived, pieces):
    size = target_ref.shape[0] // pieces
    return [
        pltpu.make_async_copy(source_ref.at[pl.ds(k * size, size)], target_ref.at[pl.ds(k * size, size)], arrived.at[k])
        for k in range(pieces)
    ]


def first_front(
    cell_ref, tokens_hbm, gain_hbm, wq_hbm, wk_hbm, wv_hbm, wo_hbm, wg_hbm, bias_hbm, stab_hbm, norm_hbm, *rest, head_size
):
    *outs, held_ref, own_ref, arrived, loaded, tokens_ref, gain_ref, weights_ref, bias_ref, stab_ref, norm_ref = rest
    columns = own_ref.shape[0]
    gates = wg_hbm.shape[1]
    sources = [tokens_hbm, gain_hbm, bias_hbm, stab_hbm.at[0], norm_hbm.at[0]]
    targets = [tokens_ref, gain_ref, bias_ref, stab_ref, norm_ref]
    for k, weight in enumerate((wq_hbm, wk_hbm, wv_hbm, wo_hbm)):
        sources.append(weight.at[0])
        targets.append(weights_ref.at[pl.ds(k * columns, columns)])
    sources.append(wg_hbm.at[0])
    targets.append(weights_ref.at[pl.ds(4 * columns, gates)])
    loads = [pltpu.make_async_copy(a, b, loaded.at[k]) for k, (a, b) in enumerate(zip(sources, targets))]
    for load in loads:
        load.start()
    fetches = fetched(cell_ref.at[0], held_ref, arrived, PIECES)
    for fetch in fetches:
        fetch.start()
    loads[0].wait()
    loads[1].wait()
    near = NEAR * columns
    device = lax.axis_index("tp")
    nearby = tokens_ref[:, pl.ds(pl.multiple_of(device // NEAR * near, near), near)].astype(F32)
    turned = pltpu.roll(nearby, (NEAR - device % NEAR) % NEAR * columns, 1).T
    own_ref[...] = turned[:columns].astype(BF16)
    current = tokens_ref[...].astype(F32)
    scale = lax.rsqrt(jnp.mean(current * current, axis=1, keepdims=True) + EPSILON)
    normed = (current * scale * gain_ref[0:1, :]).astype(BF16)
    for load in loads[2:]:
        load.wait()
    dots = lax.dot_general(weights_ref[...], normed, (((1,), (1,)), ((), ())), preferred_element_type=F32)
    front_rest(0, dots, bias_ref, stab_ref, norm_ref, *outs, head_size=head_size)
    for fetch in fetches:
        fetch.wait()


def later_front(own_ref, first_ref, second_ref, third_ref, gain_ref, wq_ref, wk_ref, wv_ref, wo_ref, wg_ref, *rest, layer, head_size):
    *rest, stage_ref, normed_ref = rest
    unpack((own_ref, first_ref, second_ref, third_ref), stage_ref)
    far, per, batch = stage_ref.shape
    current = stage_ref[...].astype(F32)
    square = jnp.sum(jnp.sum(current * current, axis=0), axis=0, keepdims=True)
    scale = lax.rsqrt(square / (far * per) + EPSILON)
    gain = jnp.concatenate([gain_ref[layer : layer + 1, i * per : (i + 1) * per] for i in range(far)]).T
    for i in range(far):
        normed_ref[i * per : (i + 1) * per, :] = (current[i] * scale * gain[:, i : i + 1]).astype(BF16)
    weights = jnp.concatenate([wq_ref[layer], wk_ref[layer], wv_ref[layer], wo_ref[layer], wg_ref[layer]])
    outs = jnp.dot(weights, normed_ref[...], preferred_element_type=F32)
    bias_ref, stab_ref, norm_ref, *made = rest
    front_rest(layer, outs, bias_ref, stab_ref.at[layer], norm_ref.at[layer], *made, head_size=head_size)


def in_hbm(*values):
    return [pltpu.with_memory_space_constraint(value, pltpu.HBM) for value in values]


def fetch_kernel(layer, cell_ref, after_ref, held_ref, arrived):
    del after_ref
    fetches = fetched(cell_ref.at[layer], held_ref, arrived, PIECES)
    for fetch in fetches:
        fetch.start()
    for fetch in fetches:
        fetch.wait()


def fetch(layer, cell, after):
    return pl.pallas_call(
        functools.partial(fetch_kernel, layer),
        out_shape=jax.ShapeDtypeStruct(cell.shape[1:], F32),
        in_specs=[anywhere()] * 2,
        out_specs=anywhere(),
        scratch_shapes=[pltpu.SemaphoreType.DMA((PIECES,))],
        compiler_params=LIMITED,
        name="fetch",
    )(*in_hbm(cell), after)


def front(layer, current, norm_gain, projections, gates, bias, stab, norm, cell):
    _, columns, width = projections[0].shape
    heads, batch = stab.shape[1:]
    head_size = cell.shape[-1]
    group = head_size // columns
    far = lax.axis_size("tp") // NEAR
    out_shape = [
        jax.ShapeDtypeStruct((group, columns + 16, 2 * batch), BF16),
        jax.ShapeDtypeStruct((columns, batch), F32),
        jax.ShapeDtypeStruct((columns, batch), F32),
        jax.ShapeDtypeStruct((8, 2 * batch), F32),
        jax.ShapeDtypeStruct((columns, batch), F32),
        jax.ShapeDtypeStruct((heads, batch), F32),
    ]
    if layer == 0:
        operands = (cell, current, norm_gain, *projections, gates, bias, stab, norm)
        return pl.pallas_call(
            functools.partial(first_front, head_size=head_size),
            out_shape=out_shape + [jax.ShapeDtypeStruct(cell.shape[1:], F32), jax.ShapeDtypeStruct((columns, batch), BF16)],
            out_specs=[near_vmem()] * len(out_shape) + [anywhere(), near_vmem()],
            in_specs=[anywhere()] * len(operands),
            scratch_shapes=[
                pltpu.SemaphoreType.DMA((PIECES,)),
                pltpu.SemaphoreType.DMA((10,)),
                pltpu.VMEM((batch, width), BF16),
                pltpu.VMEM(norm_gain.shape, F32),
                pltpu.VMEM((4 * columns + 2 * heads, width), BF16),
                pltpu.VMEM(bias.shape, F32),
                pltpu.VMEM((heads, batch), F32),
                pltpu.VMEM((columns, batch), F32),
            ],
            compiler_params=LIMITED,
            name="front_first",
        )(*in_hbm(*operands))
    per = width // far
    operands = (*current, norm_gain, *projections, gates, bias, stab, norm)
    return pl.pallas_call(
        functools.partial(later_front, layer=layer, head_size=head_size),
        out_shape=out_shape,
        out_specs=[near_vmem()] * len(out_shape),
        in_specs=[near_vmem()] * len(operands),
        scratch_shapes=[
            pltpu.VMEM((far, per, batch), BF16),
            pltpu.VMEM((width, batch), BF16),
        ],
        compiler_params=LIMITED,
        name="front_later",
    )(*operands)


def head_rows(everyone_ref, columns):
    group, _, lanes = everyone_ref.shape
    return everyone_ref[:, :columns, :].astype(F32).reshape(group * columns, lanes)


def read_kernel(everyone_ref, value_ref, open_ref, rows_ref, cell_ref, copies_ref, turned_ref):
    columns, batch = value_ref.shape
    half_keys = cell_ref.shape[2] // 2
    both = head_rows(everyone_ref, columns)
    turned_ref[...] = both.T
    product = jnp.sum(both[:, :batch] * both[:, batch:], axis=0, keepdims=True)
    lane = lax.broadcasted_iota(jnp.int32, (columns, batch), 1)

    def some(step, sums):
        for i in range(UNROLLED):
            b = step * UNROLLED + i
            products = cell_ref[b] * turned_ref[pl.ds(b, 1), :]
            folded = products[:, :half_keys] + products[:, half_keys:]
            sums = jnp.where(lane == b, jnp.sum(folded, axis=1, keepdims=True), sums)
        return sums

    sums = lax.fori_loop(0, batch // UNROLLED, some, jnp.zeros((columns, batch), F32))
    parts = jnp.sum(everyone_ref[:, columns:, :].astype(F32), axis=0)
    denom = parts[0:1, :batch] + parts[0:1, batch:] + parts[1:2, :batch]
    decay = rows_ref[0:1, :batch]
    weight = rows_ref[0:1, batch:]
    floor = rows_ref[1:2, :batch]
    numer = decay * sums + value_ref[...] * (weight * product)
    readout = numer / jnp.maximum(jnp.abs(denom), floor)
    branch = (open_ref[...] * readout).astype(BF16)
    half = columns // 2
    packed = jnp.concatenate([branch[:half], branch[half:]], axis=1)
    copies_ref[...] = jnp.broadcast_to(packed[None], copies_ref.shape)


def read(everyone, value, opened, rows, held):
    columns, batch = value.shape
    far = lax.axis_size("tp") // NEAR
    out_shape = jax.ShapeDtypeStruct((far, columns // 2, 2 * batch), BF16)
    operands = (everyone, value, opened, rows, held)
    return pl.pallas_call(
        read_kernel,
        out_shape=out_shape,
        in_specs=[near_vmem()] * len(operands),
        out_specs=near_vmem(),
        scratch_shapes=[pltpu.VMEM((2 * batch, held.shape[-1]), F32)],
        compiler_params=LIMITED,
        name="read",
    )(*operands)


def update_kernel(layer, layers, everyone_ref, value_ref, rows_ref, held_ref, *rest):
    *rest, fresh_ref, turned_ref, decay_ref, written = rest
    columns, batch = value_ref.shape
    keys = held_ref.shape[-1]
    if layers:
        norm_refs, stab_refs = rest[:layers], rest[layers : 2 * layers]
        *_, cells_ref, norms_ref, stabs_ref = rest
        for k in range(layers):
            norms_ref[k] = norm_refs[k][...]
            stabs_ref[k] = stab_refs[k][...]
    else:
        cells_ref = rest[-1]
    turned_ref[...] = head_rows(everyone_ref, columns).T
    decay_ref[...] = jnp.broadcast_to(rows_ref[0:1, :], (2 * batch, 2 * batch)).T
    added = value_ref[...] * rows_ref[0:1, batch:]
    chunk = batch // CHUNKS
    writes = []
    for k in range(CHUNKS):
        for b in range(k * chunk, (k + 1) * chunk):
            key = turned_ref[batch + b : batch + b + 1, :]
            decay = decay_ref[b : b + 1, :]
            decay = jnp.concatenate([decay] * (keys // decay.shape[1]), axis=1)
            fresh_ref[b] = decay * held_ref[b] + added[:, b : b + 1] * key
        part = pl.ds(k * chunk, chunk)
        writes.append(pltpu.make_async_copy(fresh_ref.at[part], cells_ref.at[layer, part], written.at[k]))
        writes[-1].start()
    for write in writes:
        write.wait()


def update(layer, layers, everyone, value, rows, held, into, small, after):
    columns, batch = value.shape
    keys = held.shape[-1]
    operands = [everyone, value, rows, held, *small]
    in_specs = [near_vmem()] * len(operands)
    out_shape = [jax.ShapeDtypeStruct((layers, *held.shape), F32)]
    out_specs = [anywhere()]
    if small:
        for each in (small[0], small[-1]):
            out_shape.append(jax.ShapeDtypeStruct((layers, *each.shape), F32))
            out_specs.append(near_vmem())
    operands.append(after)
    in_specs.append(anywhere())
    aliases = {}
    if into is not None:
        aliases = {len(operands): 0}
        operands.extend(in_hbm(into))
        in_specs.append(anywhere())
    return pl.pallas_call(
        functools.partial(update_kernel, layer, len(small) // 2),
        out_shape=out_shape,
        in_specs=in_specs,
        out_specs=out_specs,
        scratch_shapes=[
            pltpu.VMEM(held.shape, F32),
            pltpu.VMEM((2 * batch, keys), F32),
            pltpu.VMEM((2 * batch, 2 * batch), F32),
            pltpu.SemaphoreType.DMA((CHUNKS,)),
        ],
        input_output_aliases=aliases,
        compiler_params=LIMITED,
        name="update",
    )(*operands)


def proj_result(layer, pieces, weight_ref, residual_ref, stage_ref):
    unpack(pieces, stage_ref)
    far, per, batch = stage_ref.shape
    summed = jnp.dot(weight_ref[layer], stage_ref[...].reshape(far * per, batch), preferred_element_type=F32)
    return (residual_ref[...].astype(F32) + summed).astype(BF16)


def proj_kernel(layer, own_ref, first_ref, second_ref, third_ref, weight_ref, residual_ref, result_ref, *rest):
    *copies, stage_ref = rest
    pieces = (own_ref, first_ref, second_ref, third_ref)
    result = proj_result(layer, pieces, weight_ref, residual_ref, stage_ref)
    result_ref[...] = result
    half = result.shape[0] // 2
    for copies_ref in copies:
        packed = jnp.concatenate([result[:half], result[half:]], axis=1)
        copies_ref[...] = jnp.broadcast_to(packed[None], copies_ref.shape)


def proj(layer, pieces, weight, residual, send):
    _, columns, width = weight.shape
    batch = residual.shape[1]
    far = lax.axis_size("tp") // NEAR
    out_shape = [jax.ShapeDtypeStruct((columns, batch), BF16)]
    operands = (*pieces, weight, residual)
    if send:
        out_shape.append(jax.ShapeDtypeStruct((far, columns // 2, 2 * batch), BF16))
    return pl.pallas_call(
        functools.partial(proj_kernel, layer),
        out_shape=out_shape,
        in_specs=[near_vmem()] * len(operands),
        out_specs=[near_vmem()] * len(out_shape),
        scratch_shapes=[pltpu.VMEM((far, width // far, batch), BF16)],
        compiler_params=LIMITED,
        name="proj",
    )(*operands)


def body(tokens, norm_gain, query_weight, key_weight, value_weight, outgate_weight, gate_weight, forget_bias, proj_weight, cell_state, normalizer, stabilizer):
    layers, columns, _ = query_weight.shape
    head_size = cell_state.shape[-1]
    group = head_size // columns
    gates = gate_weight.transpose(0, 2, 1)
    stab = stabilizer.transpose(0, 2, 1)
    norm = normalizer.transpose(0, 2, 1)
    projections = (query_weight, key_weight, value_weight, outgate_weight)
    current = tokens
    cells = None
    held = [None] * layers
    norms, stabs = [], []
    for layer in range(layers):
        last = layer + 1 == layers
        message, value, opened, rows, new_norm, new_stab, *more = front(
            layer, current, norm_gain, projections, gates, forget_bias, stab, norm, cell_state
        )
        norms.append(new_norm)
        stabs.append(new_stab)
        if layer == 0:
            held[0], residual = more
        everyone = exchanged(message, near_groups(lax.axis_size("tp"), group))
        copies = read(everyone, value, opened, rows, held[layer])
        small = (*norms, *stabs) if last else ()
        write = functools.partial(update, layer, layers, everyone, value, rows, held[layer], cells, small)
        if last:
            pieces, states = gathered(copies, write)
            (residual,) = proj(layer, pieces, proj_weight, residual, False)
        else:
            pieces, held[layer + 1] = gathered(copies, functools.partial(fetch, layer + 1, cell_state))
            residual, copies = proj(layer, pieces, proj_weight, residual, True)
            current, (cells,) = gathered(copies, write)
    cells, norms, stabs = states
    return (residual.T, cells, norms.transpose(0, 2, 1), stabs.transpose(0, 2, 1))


def solution(mesh):
    return jax.shard_map(
        body,
        mesh=mesh,
        in_specs=(
            P("grp", None),
            P(),
            P(None, "tp", None),
            P(None, "tp", None),
            P(None, "tp", None),
            P(None, "tp", None),
            P(),
            P(),
            P(None, "tp", None),
            P(None, "grp", "tp", None),
            P(None, "grp", "tp"),
            P(None, "grp", None),
        ),
        out_specs=(
            P("grp", "tp"),
            P(None, "grp", "tp", None),
            P(None, "grp", "tp"),
            P(None, "grp", None),
        ),
        check_vma=False,
    )
```

```python
import functools

import jax
import jax.numpy as jnp
from jax import lax
from jax.experimental import pallas as pl
from jax.experimental.pallas import tpu as pltpu
from jax.sharding import PartitionSpec as P


EPSILON = 1e-06
NEAR = 4
CHUNKS = 4
UNROLLED = 32
PIECES = 4
F32 = jnp.float32
BF16 = jnp.bfloat16
LIMITED = pltpu.CompilerParams(vmem_limit_bytes=16 * 2**20)


def near_groups(total, size):
    return [[first + i for i in range(size)] for first in range(0, total, size)]


def far_groups(total, stride):
    return [list(range(first, total, stride)) for first in range(stride)]


def exchanged(copies, groups):
    return lax.all_to_all(copies, "tp", 0, 0, tiled=True, axis_index_groups=groups)


def from_partner(value, mask):
    pairs = [(source, source ^ mask) for source in range(lax.axis_size("tp"))]
    return lax.ppermute(value, "tp", pairs)


def gathered(copies, meanwhile=None):
    count, rows, lanes = copies.shape
    far = exchanged(copies, far_groups(lax.axis_size("tp"), NEAR))
    own = far.reshape(count * rows, lanes)
    second = from_partner(own, 2)
    third = from_partner(own, 3)
    first = from_partner(own, 1)
    made = None
    if meanwhile is not None:
        first, second, third, made = lax.optimization_barrier((first, second, third, meanwhile(own)))
    return (own, first, second, third), made


def anywhere():
    return pl.BlockSpec(memory_space=pl.ANY)


def near_vmem():
    return pl.BlockSpec(memory_space=pltpu.VMEM)


def unpack(pieces, stage_ref):
    own = lax.axis_index("tp") % NEAR
    far, per, batch = stage_ref.shape
    half = per // (2 * NEAR)
    for flip, piece in enumerate(pieces):
        start = pl.multiple_of((own ^ flip) * 2 * half, 2 * half)
        both = piece[...].reshape(far, half, 2 * batch)
        stage_ref[:, pl.ds(start, half), :] = both[:, :, :batch]
        stage_ref[:, pl.ds(start + half, half), :] = both[:, :, batch:]


def front_rest(layer, outs, bias_ref, stab_ref, norm_ref, message_ref, value_ref, open_ref, rows_ref, new_norm_ref, new_stab_ref, head_size):
    columns, batch = norm_ref.shape
    heads = stab_ref.shape[0]
    head = lax.axis_index("tp") // (head_size // columns)
    query = outs[:columns].astype(BF16)
    keys = (outs[columns : 2 * columns] * head_size ** (-0.5)).astype(BF16)
    value_ref[...] = outs[2 * columns : 3 * columns].astype(BF16).astype(F32)
    open_ref[...] = jax.nn.sigmoid(outs[3 * columns : 4 * columns].astype(BF16).astype(F32))
    in_gate = outs[4 * columns : 4 * columns + heads]
    row = lax.broadcasted_iota(jnp.int32, (heads, heads), 0)
    col = lax.broadcasted_iota(jnp.int32, (heads, heads), 1)
    spread = jnp.broadcast_to(bias_ref[layer : layer + 1, :], (heads, heads))
    bias = jnp.sum(jnp.where(row == col, spread, 0.0), axis=1, keepdims=True)
    forget = outs[4 * columns + heads :] + bias
    log_forget = jnp.minimum(forget, 0.0) - jnp.log1p(jnp.exp(-jnp.abs(forget)))
    shifted = log_forget + stab_ref[...]
    new_stab = jnp.maximum(shifted, in_gate)
    decay = jnp.exp(shifted - new_stab)
    weight = jnp.exp(in_gate - new_stab)
    floor = jnp.exp(-new_stab)
    mine = lax.broadcasted_iota(jnp.int32, (heads, batch), 0) == head

    def own(table):
        return jnp.sum(jnp.where(mine, table, 0.0), axis=0, keepdims=True)

    decay, weight, floor = own(decay), own(weight), own(floor)
    new_norm = decay * norm_ref[...] + weight * keys.astype(F32)
    part = jnp.sum(query.astype(F32) * new_norm, axis=0, keepdims=True)
    high = part.astype(BF16).astype(F32)
    middle = (part - high).astype(BF16).astype(F32)
    low = part - high - middle
    none = jnp.zeros_like(low)
    extra = jnp.concatenate(
        [jnp.concatenate([high, middle], axis=1), jnp.concatenate([low, none], axis=1), jnp.zeros((14, 2 * batch), F32)]
    ).astype(BF16)
    message = jnp.concatenate([jnp.concatenate([query, keys], axis=1), extra])
    message_ref[...] = jnp.broadcast_to(message[None], message_ref.shape)
    rows_ref[...] = jnp.concatenate(
        [jnp.concatenate([decay, weight], axis=1), jnp.concatenate([floor, none], axis=1), jnp.zeros((6, 2 * batch), F32)]
    )
    new_norm_ref[...] = new_norm
    new_stab_ref[...] = new_stab


def fetched(source_ref, target_ref, arrived, pieces):
    size = target_ref.shape[0] // pieces
    return [
        pltpu.make_async_copy(source_ref.at[pl.ds(k * size, size)], target_ref.at[pl.ds(k * size, size)], arrived.at[k])
        for k in range(pieces)
    ]


def first_front(
    cell_ref, tokens_hbm, gain_hbm, wq_hbm, wk_hbm, wv_hbm, wo_hbm, wg_hbm, bias_hbm, stab_hbm, norm_hbm, *rest, head_size
):
    *outs, held_ref, own_ref, arrived, loaded, tokens_ref, gain_ref, weights_ref, bias_ref, stab_ref, norm_ref = rest
    columns = own_ref.shape[0]
    gates = wg_hbm.shape[1]
    sources = [tokens_hbm, gain_hbm, bias_hbm, stab_hbm.at[0], norm_hbm.at[0]]
    targets = [tokens_ref, gain_ref, bias_ref, stab_ref, norm_ref]
    for k, weight in enumerate((wq_hbm, wk_hbm, wv_hbm, wo_hbm)):
        sources.append(weight.at[0])
        targets.append(weights_ref.at[pl.ds(k * columns, columns)])
    sources.append(wg_hbm.at[0])
    targets.append(weights_ref.at[pl.ds(4 * columns, gates)])
    loads = [pltpu.make_async_copy(a, b, loaded.at[k]) for k, (a, b) in enumerate(zip(sources, targets))]
    for load in loads:
        load.start()
    fetches = fetched(cell_ref.at[0], held_ref, arrived, PIECES)
    for fetch in fetches:
        fetch.start()
    loads[0].wait()
    loads[1].wait()
    near = NEAR * columns
    device = lax.axis_index("tp")
    nearby = tokens_ref[:, pl.ds(pl.multiple_of(device // NEAR * near, near), near)].astype(F32)
    turned = pltpu.roll(nearby, (NEAR - device % NEAR) % NEAR * columns, 1).T
    own_ref[...] = turned[:columns].astype(BF16)
    current = tokens_ref[...].astype(F32)
    scale = lax.rsqrt(jnp.mean(current * current, axis=1, keepdims=True) + EPSILON)
    normed = (current * scale * gain_ref[0:1, :]).astype(BF16)
    for load in loads[2:]:
        load.wait()
    dots = lax.dot_general(weights_ref[...], normed, (((1,), (1,)), ((), ())), preferred_element_type=F32)
    front_rest(0, dots, bias_ref, stab_ref, norm_ref, *outs, head_size=head_size)
    for fetch in fetches:
        fetch.wait()


def later_front(own_ref, first_ref, second_ref, third_ref, gain_ref, wq_ref, wk_ref, wv_ref, wo_ref, wg_ref, *rest, layer, head_size):
    *rest, stage_ref, normed_ref = rest
    unpack((own_ref, first_ref, second_ref, third_ref), stage_ref)
    far, per, _ = stage_ref.shape
    current = stage_ref[...].astype(F32)
    square = jnp.sum(jnp.sum(current * current, axis=0), axis=0, keepdims=True)
    scale = lax.rsqrt(square / (far * per) + EPSILON)
    gain = jnp.concatenate([gain_ref[layer : layer + 1, i * per : (i + 1) * per] for i in range(far)]).T
    for i in range(far):
        normed_ref[i * per : (i + 1) * per, :] = (current[i] * scale * gain[:, i : i + 1]).astype(BF16)
    weights = jnp.concatenate([wq_ref[layer], wk_ref[layer], wv_ref[layer], wo_ref[layer], wg_ref[layer]])
    outs = jnp.dot(weights, normed_ref[...], preferred_element_type=F32)
    bias_ref, stab_ref, norm_ref, *made = rest
    front_rest(layer, outs, bias_ref, stab_ref.at[layer], norm_ref.at[layer], *made, head_size=head_size)


def in_hbm(*values):
    return [pltpu.with_memory_space_constraint(value, pltpu.HBM) for value in values]


def fetch_kernel(layer, cell_ref, after_ref, held_ref, arrived):
    del after_ref
    fetches = fetched(cell_ref.at[layer], held_ref, arrived, PIECES)
    for fetch in fetches:
        fetch.start()
    for fetch in fetches:
        fetch.wait()


def fetch(layer, cell, after):
    return pl.pallas_call(
        functools.partial(fetch_kernel, layer),
        out_shape=jax.ShapeDtypeStruct(cell.shape[1:], F32),
        in_specs=[anywhere()] * 2,
        out_specs=anywhere(),
        scratch_shapes=[pltpu.SemaphoreType.DMA((PIECES,))],
        compiler_params=LIMITED,
        name="fetch",
    )(*in_hbm(cell), after)


def front(layer, current, norm_gain, projections, gates, bias, stab, norm, cell):
    _, columns, width = projections[0].shape
    heads, batch = stab.shape[1:]
    head_size = cell.shape[-1]
    group = head_size // columns
    far = lax.axis_size("tp") // NEAR
    out_shape = [
        jax.ShapeDtypeStruct((group, columns + 16, 2 * batch), BF16),
        jax.ShapeDtypeStruct((columns, batch), F32),
        jax.ShapeDtypeStruct((columns, batch), F32),
        jax.ShapeDtypeStruct((8, 2 * batch), F32),
        jax.ShapeDtypeStruct((columns, batch), F32),
        jax.ShapeDtypeStruct((heads, batch), F32),
    ]
    if layer == 0:
        operands = (cell, current, norm_gain, *projections, gates, bias, stab, norm)
        return pl.pallas_call(
            functools.partial(first_front, head_size=head_size),
            out_shape=out_shape + [jax.ShapeDtypeStruct(cell.shape[1:], F32), jax.ShapeDtypeStruct((columns, batch), BF16)],
            out_specs=[near_vmem()] * len(out_shape) + [anywhere(), near_vmem()],
            in_specs=[anywhere()] * len(operands),
            scratch_shapes=[
                pltpu.SemaphoreType.DMA((PIECES,)),
                pltpu.SemaphoreType.DMA((10,)),
                pltpu.VMEM((batch, width), BF16),
                pltpu.VMEM(norm_gain.shape, F32),
                pltpu.VMEM((4 * columns + 2 * heads, width), BF16),
                pltpu.VMEM(bias.shape, F32),
                pltpu.VMEM((heads, batch), F32),
                pltpu.VMEM((columns, batch), F32),
            ],
            compiler_params=LIMITED,
            name="front_first",
        )(*in_hbm(*operands))
    per = width // far
    operands = (*current, norm_gain, *projections, gates, bias, stab, norm)
    return pl.pallas_call(
        functools.partial(later_front, layer=layer, head_size=head_size),
        out_shape=out_shape,
        out_specs=[near_vmem()] * len(out_shape),
        in_specs=[near_vmem()] * len(operands),
        scratch_shapes=[
            pltpu.VMEM((far, per, batch), BF16),
            pltpu.VMEM((width, batch), BF16),
        ],
        compiler_params=LIMITED,
        name="front_later",
    )(*operands)


def head_rows(everyone_ref, columns):
    group, _, lanes = everyone_ref.shape
    return everyone_ref[:, :columns, :].astype(F32).reshape(group * columns, lanes)


def read_kernel(everyone_ref, value_ref, open_ref, rows_ref, cell_ref, copies_ref, turned_ref):
    columns, batch = value_ref.shape
    half_keys = cell_ref.shape[2] // 2
    both = head_rows(everyone_ref, columns)
    turned_ref[...] = both.T
    product = jnp.sum(both[:, :batch] * both[:, batch:], axis=0, keepdims=True)
    lane = lax.broadcasted_iota(jnp.int32, (columns, batch), 1)

    def some(step, sums):
        for i in range(UNROLLED):
            b = step * UNROLLED + i
            products = cell_ref[b] * turned_ref[pl.ds(b, 1), :]
            folded = products[:, :half_keys] + products[:, half_keys:]
            sums = jnp.where(lane == b, jnp.sum(folded, axis=1, keepdims=True), sums)
        return sums

    sums = lax.fori_loop(0, batch // UNROLLED, some, jnp.zeros((columns, batch), F32))
    parts = jnp.sum(everyone_ref[:, columns:, :].astype(F32), axis=0)
    denom = parts[0:1, :batch] + parts[0:1, batch:] + parts[1:2, :batch]
    decay = rows_ref[0:1, :batch]
    weight = rows_ref[0:1, batch:]
    floor = rows_ref[1:2, :batch]
    numer = decay * sums + value_ref[...] * (weight * product)
    readout = numer / jnp.maximum(jnp.abs(denom), floor)
    branch = (open_ref[...] * readout).astype(BF16)
    half = columns // 2
    packed = jnp.concatenate([branch[:half], branch[half:]], axis=1)
    copies_ref[...] = jnp.broadcast_to(packed[None], copies_ref.shape)


def read(everyone, value, opened, rows, held):
    columns, batch = value.shape
    far = lax.axis_size("tp") // NEAR
    out_shape = jax.ShapeDtypeStruct((far, columns // 2, 2 * batch), BF16)
    operands = (everyone, value, opened, rows, held)
    return pl.pallas_call(
        read_kernel,
        out_shape=out_shape,
        in_specs=[near_vmem()] * len(operands),
        out_specs=near_vmem(),
        scratch_shapes=[pltpu.VMEM((2 * batch, held.shape[-1]), F32)],
        compiler_params=LIMITED,
        name="read",
    )(*operands)


def update_kernel(layer, layers, everyone_ref, value_ref, rows_ref, held_ref, *rest):
    *rest, fresh_ref, turned_ref, decay_ref, written = rest
    columns, batch = value_ref.shape
    keys = held_ref.shape[-1]
    if layers:
        norm_refs, stab_refs = rest[:layers], rest[layers : 2 * layers]
        *_, cells_ref, norms_ref, stabs_ref = rest
        for k in range(layers):
            norms_ref[k] = norm_refs[k][...]
            stabs_ref[k] = stab_refs[k][...]
    else:
        cells_ref = rest[-1]
    turned_ref[...] = head_rows(everyone_ref, columns).T
    decay_ref[...] = jnp.broadcast_to(rows_ref[0:1, :], (2 * batch, 2 * batch)).T
    added = value_ref[...] * rows_ref[0:1, batch:]
    chunk = batch // CHUNKS
    writes = []
    for k in range(CHUNKS):
        for b in range(k * chunk, (k + 1) * chunk):
            key = turned_ref[batch + b : batch + b + 1, :]
            decay = decay_ref[b : b + 1, :]
            decay = jnp.concatenate([decay] * (keys // decay.shape[1]), axis=1)
            fresh_ref[b] = decay * held_ref[b] + added[:, b : b + 1] * key
        part = pl.ds(k * chunk, chunk)
        writes.append(pltpu.make_async_copy(fresh_ref.at[part], cells_ref.at[layer, part], written.at[k]))
        writes[-1].start()
    for write in writes:
        write.wait()


def update(layer, layers, everyone, value, rows, held, into, small, after):
    _, batch = value.shape
    keys = held.shape[-1]
    operands = [everyone, value, rows, held, *small]
    in_specs = [near_vmem()] * len(operands)
    out_shape = [jax.ShapeDtypeStruct((layers, *held.shape), F32)]
    out_specs = [anywhere()]
    if small:
        for each in (small[0], small[-1]):
            out_shape.append(jax.ShapeDtypeStruct((layers, *each.shape), F32))
            out_specs.append(near_vmem())
    operands.append(after)
    in_specs.append(anywhere())
    aliases = {}
    if into is not None:
        aliases = {len(operands): 0}
        operands.extend(in_hbm(into))
        in_specs.append(anywhere())
    return pl.pallas_call(
        functools.partial(update_kernel, layer, len(small) // 2),
        out_shape=out_shape,
        in_specs=in_specs,
        out_specs=out_specs,
        scratch_shapes=[
            pltpu.VMEM(held.shape, F32),
            pltpu.VMEM((2 * batch, keys), F32),
            pltpu.VMEM((2 * batch, 2 * batch), F32),
            pltpu.SemaphoreType.DMA((CHUNKS,)),
        ],
        input_output_aliases=aliases,
        compiler_params=LIMITED,
        name="update",
    )(*operands)


def proj_result(layer, pieces, weight_ref, residual_ref, stage_ref):
    unpack(pieces, stage_ref)
    far, per, batch = stage_ref.shape
    summed = jnp.dot(weight_ref[layer], stage_ref[...].reshape(far * per, batch), preferred_element_type=F32)
    return (residual_ref[...].astype(F32) + summed).astype(BF16)


def proj_kernel(layer, own_ref, first_ref, second_ref, third_ref, weight_ref, residual_ref, result_ref, *rest):
    *copies, stage_ref = rest
    pieces = (own_ref, first_ref, second_ref, third_ref)
    result = proj_result(layer, pieces, weight_ref, residual_ref, stage_ref)
    result_ref[...] = result
    half = result.shape[0] // 2
    for copies_ref in copies:
        packed = jnp.concatenate([result[:half], result[half:]], axis=1)
        copies_ref[...] = jnp.broadcast_to(packed[None], copies_ref.shape)


def proj(layer, pieces, weight, residual, send):
    _, columns, width = weight.shape
    batch = residual.shape[1]
    far = lax.axis_size("tp") // NEAR
    out_shape = [jax.ShapeDtypeStruct((columns, batch), BF16)]
    operands = (*pieces, weight, residual)
    if send:
        out_shape.append(jax.ShapeDtypeStruct((far, columns // 2, 2 * batch), BF16))
    return pl.pallas_call(
        functools.partial(proj_kernel, layer),
        out_shape=out_shape,
        in_specs=[near_vmem()] * len(operands),
        out_specs=[near_vmem()] * len(out_shape),
        scratch_shapes=[pltpu.VMEM((far, width // far, batch), BF16)],
        compiler_params=LIMITED,
        name="proj",
    )(*operands)


def body(tokens, norm_gain, query_weight, key_weight, value_weight, outgate_weight, gate_weight, forget_bias, proj_weight, cell_state, normalizer, stabilizer):
    layers, columns, _ = query_weight.shape
    head_size = cell_state.shape[-1]
    group = head_size // columns
    gates = gate_weight.transpose(0, 2, 1)
    stab = stabilizer.transpose(0, 2, 1)
    norm = normalizer.transpose(0, 2, 1)
    projections = (query_weight, key_weight, value_weight, outgate_weight)
    current = tokens
    cells = None
    held = [None] * layers
    norms, stabs = [], []
    for layer in range(layers):
        last = layer + 1 == layers
        message, value, opened, rows, new_norm, new_stab, *more = front(
            layer, current, norm_gain, projections, gates, forget_bias, stab, norm, cell_state
        )
        norms.append(new_norm)
        stabs.append(new_stab)
        if layer == 0:
            held[0], residual = more
        everyone = exchanged(message, near_groups(lax.axis_size("tp"), group))
        copies = read(everyone, value, opened, rows, held[layer])
        small = (*norms, *stabs) if last else ()
        write = functools.partial(update, layer, layers, everyone, value, rows, held[layer], cells, small)
        if last:
            pieces, states = gathered(copies, write)
            (residual,) = proj(layer, pieces, proj_weight, residual, False)
        else:
            pieces, held[layer + 1] = gathered(copies, functools.partial(fetch, layer + 1, cell_state))
            residual, copies = proj(layer, pieces, proj_weight, residual, True)
            current, (cells,) = gathered(copies, write)
    cells, norms, stabs = states
    return (residual.T, cells, norms.transpose(0, 2, 1), stabs.transpose(0, 2, 1))


def solution(mesh):
    return jax.shard_map(
        body,
        mesh=mesh,
        in_specs=(
            P("grp", None),
            P(),
            P(None, "tp", None),
            P(None, "tp", None),
            P(None, "tp", None),
            P(None, "tp", None),
            P(),
            P(),
            P(None, "tp", None),
            P(None, "grp", "tp", None),
            P(None, "grp", "tp"),
            P(None, "grp", None),
        ),
        out_specs=(
            P("grp", "tp"),
            P(None, "grp", "tp", None),
            P(None, "grp", "tp"),
            P(None, "grp", None),
        ),
        check_vma=False,
    )
```
